32 devices in a mesh: rep: 2 (over y), fs: 4 (over z), tp: 4 (over x, core).
Axes of the slice: x: 2, y: 2, z: 4, core: 2. Of those that a mesh axis runs over, the one named last changes fastest.
Arguments:
- gate_pre: bfloat16 [8192, 3072], P(('rep', 'fs'), 'tp'), may hold values from -6 to 6
- up_pre: bfloat16 [8192, 3072], P(('rep', 'fs'), 'tp'), may hold values from -6 to 6
- out_grad: bfloat16 [8192, 2048], P(('rep', 'fs')), may hold values from -8 to 8
- w_down: bfloat16 [3072, 2048], P('tp', 'fs'), may hold values from -0.109375 to 0.109375
Outputs:
- d_gate: bfloat16 [8192, 3072], P(('rep', 'fs'), 'tp')
- d_up: bfloat16 [8192, 3072], P(('rep', 'fs'), 'tp')
- grad_down: float32 [3072, 2048], P('tp', 'fs')
- row_energy: float32 [3072], P('tp')
The draws below stay inside these ranges and needn't reach their ends.
All inputs are finite; a program needn't handle non-finite values.
Results may differ from the reference program's by a relative error of at most 0.0034.
Values may be sent and summed in bfloat16 or wider, within the bound.
A program may use at most 64 MiB of HBM per device.

```python
import jax
import jax.numpy as jnp
from jax import lax

D = 2048
FF = 3072
TOK_DEV = 1024
TOKENS = 8192


def raised(result, stream_key, source, target, shards_of, factor):
    def block_of(dim):
        return (jnp.arange(result.shape[dim]) // (result.shape[dim] // shards_of)).reshape((-1,) + (1,) * (result.ndim - 1 - dim))

    first = jax.random.permutation(stream_key, shards_of)[block_of(target)]
    second = (block_of(target) + shards_of // 2) % shards_of
    return jnp.where((block_of(source) == first) | (block_of(source) == second), factor * result, result)


def shard_levels(stream_key, dims, shards, least, top_value):
    factor_of = 1.0
    for axis_at, blocks in shards:
        steps = jax.random.uniform(jax.random.fold_in(jax.random.fold_in(stream_key, 6), axis_at), (blocks,), jnp.float32, least / len(shards), top_value / len(shards))
        factor_of = factor_of * jnp.repeat(jnp.exp(steps), dims[axis_at] // blocks).reshape((-1,) + (1,) * (len(dims) - 1 - axis_at))
    return factor_of


def noise(own_key, extent, deviation, reach, pieces=(), held_as=jnp.bfloat16):
    array = deviation * jax.random.normal(own_key, extent, jnp.float32)
    if pieces:
        array = array * shard_levels(own_key, extent, pieces, -0.22, 0.18)
    return jnp.clip(array, -reach, reach).astype(held_as)


def bell_draw_with(key, extent, spread, reach, split, heavy, dtype=jnp.bfloat16):
    values = spread * jax.random.normal(key, extent, jnp.float32)
    if split:
        values = values * shard_levels(key, extent, split, -0.22, 0.18)
    return jnp.clip(raised(values, jax.random.fold_in(key, 3), *heavy), -reach, reach).astype(dtype)


def setup_inputs(seed: int = 0) -> dict:
    key_of = jax.random.split(jax.random.key(seed), 5)
    return {
        "gate_pre": noise(key_of[0], (TOKENS, FF), 1.0, 6.0, ((0, 8), (1, 4))),
        "up_pre": noise(key_of[1], (TOKENS, FF), 1.0, 6.0, ((0, 8), (1, 4))),
        "out_grad": bell_draw_with(key_of[2], (TOKENS, D), 1.0, 8.0, ((0, 8),), (0, 1, 8, 2.0)),
        "w_down": noise(key_of[3], (FF, D), FF ** -0.5, 0.109375, ((0, 4), (1, 4))),
    }


def reference(gate_pre, up_pre, out_grad, w_down):
    blocks = TOKENS // TOK_DEV
    gate_blocks = gate_pre.reshape(blocks, TOK_DEV, FF)
    up_blocks = up_pre.reshape(blocks, TOK_DEV, FF)
    grad_blocks = out_grad.reshape(blocks, TOK_DEV, D)

    def step(total, items):
        gate_rows, up_rows, cot_rows = items
        gate_f = gate_rows.astype(jnp.float32)
        up_f = up_rows.astype(jnp.float32)
        sig = jax.nn.sigmoid(gate_f)
        act = gate_f * sig
        hidden = (act * up_f).astype(jnp.bfloat16)
        dhid = jnp.dot(cot_rows, w_down.T, preferred_element_type=jnp.float32)
        d_up = (dhid * act).astype(jnp.bfloat16)
        d_gate = (dhid * up_f * sig * (1.0 + gate_f * (1.0 - sig))).astype(jnp.bfloat16)
        total = total + jnp.dot(hidden.T, cot_rows, preferred_element_type=jnp.float32)
        return total, (d_gate, d_up)

    start = jnp.zeros((FF, D), jnp.float32)
    summed, outs = lax.scan(step, start, (gate_blocks, up_blocks, grad_blocks))
    grad_down = summed * (float(TOKENS) ** -0.5)
    row_energy = jnp.sum(grad_down * grad_down, axis=1) / D
    d_gate = outs[0].reshape(TOKENS, FF)
    d_up = outs[1].reshape(TOKENS, FF)
    return d_gate, d_up, grad_down, row_energy
```

```python
import functools

import jax
import jax.numpy as jnp
from jax import lax
from jax.experimental import pallas as pl
from jax.experimental.pallas import tpu as pltpu
from jax.sharding import PartitionSpec as P

MESH = pl.DeviceIdType.MESH
F32 = jnp.float32
BF16 = jnp.bfloat16
PIECES = 24
SPLIT = 7
LAG = 2
LOADS = 4
BEFORE = 2
VMEM_LIMIT = 52 * 1024 * 1024


def plain(gate_pre, up_pre, out_grad, w_down):
    gate_f = gate_pre.astype(F32)
    up_f = up_pre.astype(F32)
    sig = jax.nn.sigmoid(gate_f)
    act = gate_f * sig
    hidden = (act * up_f).astype(BF16)
    tokens_all = out_grad.shape[0] * lax.axis_size("rep") * lax.axis_size("fs")
    factor = float(tokens_all) ** (-0.5)
    weight_whole = lax.all_gather(w_down, "fs", axis=1, tiled=True)
    dhid = lax.dot_general(out_grad, weight_whole, (((1,), (1,)), ((), ())), preferred_element_type=F32)
    d_up = (dhid * act).astype(BF16)
    d_gate = (dhid * up_f * sig * (1.0 + gate_f * (1.0 - sig))).astype(BF16)
    shard = lax.psum_scatter(
        lax.dot_general(out_grad, hidden, (((0,), (0,)), ((), ())), preferred_element_type=F32),
        "fs",
        scatter_dimension=0,
        tiled=True,
    )
    shard = lax.psum(shard, "rep")
    grad_down = shard.T * factor
    energy = lax.psum(jnp.sum(grad_down * grad_down, axis=1), "fs") / out_grad.shape[1]
    return (d_gate, d_up, grad_down, energy)


def kernel(
    n, factor, width,
    g_hbm, u_hbm, og_hbm, w_hbm,
    dg, du, gd, en_ref,
    g, u, og, w, hid, part, dhid, zsend, zrecv, ysend, yrecv, fsend, frecv,
    lanes_u, lanes_s, esu, eru, ess, ers,
    in_sem, og_sem, zs_sem, zr_sem, as_sem, ar_sem, ys_sem, yr_sem, fs_sem, fr_sem,
    us_sem, ur_sem, ss_sem, sr_sem,
):
    rep = lax.axis_index("rep")
    k = lax.axis_index("fs")
    mate = 1 - rep
    cols = w.shape[3]
    rows = w.shape[2]
    hidden_units = g.shape[1]
    tokens = g.shape[0]
    count = PIECES - SPLIT
    free = PIECES - 2 * SPLIT
    pairs = count // 2
    chunk = tokens // LOADS

    def piece(c):
        return c + jnp.where(c < free, 2 * SPLIT, rep * SPLIT - free)

    def loop(lo, hi, body):
        lax.fori_loop(lo, hi, lambda i, x: (body(i), x)[1], 0)

    def steps(lo, hi, body):
        loop(lo, min(hi, pairs), lambda i: body(2 * i, 2, i))
        if hi > pairs:
            body(k * 0 + 2 * pairs, 1, k * 0 + pairs)

    end = pairs + count % 2
    low = jnp.minimum(k, n - 1 - k)

    def chosen(i):
        far = jnp.where(i < n - 1 - low, n - 1 - i, jnp.where(i < n - 1, i - (n - 1 - low), low))
        return jnp.where(2 * k >= n, n - 1 - far, far)

    def rows_at(i):
        return pl.ds(pl.multiple_of(i * chunk, chunk), chunk)

    def in_g(i):
        return pltpu.make_async_copy(g_hbm.at[rows_at(i)], g.at[rows_at(i)], in_sem.at[1 + i])

    def in_u(i):
        return pltpu.make_async_copy(u_hbm.at[rows_at(i)], u.at[rows_at(i)], in_sem.at[1 + LOADS + i])

    def in_og(j):
        part_of = pl.ds(pl.multiple_of(j * cols, cols), cols)
        return pltpu.make_async_copy(og_hbm.at[:, part_of], og.at[j], og_sem.at[j])

    at = (k, n - 1 - k)
    sign = (1, -1)

    barrier = pltpu.get_barrier_semaphore()
    for d in range(2):

        @pl.when(at[d] < n - 1)
        def _():
            pl.semaphore_signal(barrier, inc=1, device_id={"fs": k + sign[d]}, device_id_type=MESH)

    pl.semaphore_signal(barrier, inc=1, device_id={"rep": mate}, device_id_type=MESH)
    in_w = pltpu.make_async_copy(w_hbm, w.at[k], in_sem.at[0])
    in_w.start()

    def load(i):
        in_g(i).start()
        in_u(i).start()

    loop(0, LOADS, load)
    loop(0, n, lambda i: in_og(chosen(i)).start())
    lanes_u[...] = jnp.zeros_like(lanes_u)
    lanes_s[...] = jnp.zeros_like(lanes_s)
    def along(d, s, i, src, dst):
        return pltpu.make_async_remote_copy(
            src_ref=src, dst_ref=dst, send_sem=zs_sem.at[d, s], recv_sem=zr_sem.at[d, s, i],
            device_id={"fs": k + sign[d]}, device_id_type=MESH,
        )

    def across(src, dst, send, recv):
        return pltpu.make_async_remote_copy(
            src_ref=src, dst_ref=dst, send_sem=send, recv_sem=recv,
            device_id={"rep": mate}, device_id_type=MESH,
        )

    def early(j):
        return across(ysend.at[j], yrecv.at[j], ys_sem.at[0], yr_sem.at[j])

    def final(c, m, i):
        return across(fsend.at[pl.ds(c, m)], frecv.at[pl.ds(c, m)], fs_sem.at[0], fr_sem.at[i])

    def crossing(j, owner, start, m):
        block = w.at[j, pl.ds(owner * SPLIT + start, m)]
        return across(block, block, as_sem.at[j], ar_sem.at[j])

    def make_hidden(i):
        in_g(i).wait()
        in_u(i).wait()
        gate = g[rows_at(i), :].astype(F32)
        act = gate * jax.nn.sigmoid(gate)
        h = (act * u[rows_at(i), :].astype(F32)).astype(BF16)
        hid[:, rows_at(i)] = h.T

    loop(0, BEFORE, make_hidden)
    pl.semaphore_wait(barrier, 1 + (k > 0).astype(jnp.int32) + (k < n - 1).astype(jnp.int32))
    in_w.wait()

    def first(c, m, i):
        for d in range(2):

            @pl.when(at[d] < n - 1)
            def _():
                block = w.at[k, pl.ds(piece(c), m)]
                along(d, 0, i, block, block).start()

    steps(0, end, first)
    loop(BEFORE, LOADS, make_hidden)

    def product(j, start, pieces):
        some = hid[pl.ds(pl.multiple_of(start * rows, rows), pieces * rows), :]
        return jnp.dot(some, og[j], preferred_element_type=F32).reshape(pieces, rows, cols)

    def make_part(i):
        j = chosen(i)
        in_og(j).wait()
        ysend[j] = product(j, mate * SPLIT, SPLIT).astype(BF16)
        early(j).start()
        part[j, pl.ds(2 * SPLIT, free)] = product(j, 2 * SPLIT, free)
        part[j, pl.ds(rep * SPLIT, SPLIT)] = product(j, rep * SPLIT, SPLIT)

    loop(0, n, make_part)

    def multiply(j, at_rows):
        return lax.dot_general(
            og[j, at_rows, :], w[j].reshape(hidden_units, cols), (((1,), (1,)), ((), ())),
            preferred_element_type=F32,
        )

    def own(i):
        at_rows = pl.ds(pl.multiple_of(i * 256, 256), 256)
        dhid[at_rows, :] = multiply(k, at_rows)

    loop(0, tokens // 256, own)

    def pass_on(s, c, m, i):
        p = piece(c)
        for d in range(2):
            place = at[d]
            some = pl.ds(c, m)

            @pl.when(place > 0)
            def _():
                along(d, s - 1, i, zsend.at[d, 0, some], zrecv.at[d, 0, some]).wait_recv()

            @pl.when(s <= place)
            def _():
                j = k - sign[d] * s
                block = w.at[j, pl.ds(p, m)]

                @pl.when(place < n - 1)
                def _():
                    along(d, s, i, block, block).start()

                @pl.when(c >= free)
                def _():
                    crossing(j, rep, c - free, m).start()

            @pl.when(s > place)
            def _():
                j = k + sign[d] * (n - s)

                @pl.when(c == free)
                def _():
                    early(j).wait_recv()

                @pl.when(c >= free)
                def _():
                    part[j, pl.ds(p, m)] += yrecv[j, pl.ds(jnp.maximum(c - free, 0), m)].astype(F32)

                if s > 1:

                    @pl.when(place > 0)
                    def _():
                        part[j, pl.ds(p, m)] += zrecv[d, s - 2, some].astype(F32)

                zsend[d, s - 1, some] = part[j, pl.ds(p, m)].astype(BF16)
                along(d, s, i, zsend.at[d, s - 1, some], zrecv.at[d, s - 1, some]).start()

    def gathered(j):
        crossing(j, mate, 0, SPLIT).wait_recv()

    halves = 2
    half = tokens // halves

    def gather(far, part_of):
        at_rows = pl.ds(pl.multiple_of(part_of * half, half), half)
        for d in range(2):

            @pl.when(at[d] >= far)
            def _():
                j = k - sign[d] * far

                @pl.when(part_of == 0)
                def _():
                    gathered(j)

                dhid[at_rows, :] += multiply(j, at_rows)

    for s in range(1, n - 1):
        steps(0, end, functools.partial(pass_on, s))
    steps(0, pairs - 2, functools.partial(pass_on, n - 1))
    loop(0, halves, functools.partial(gather, 1))
    steps(pairs - 2, end, functools.partial(pass_on, n - 1))

    def put(p, m, value, lanes):
        gd[pl.ds(p, m)] = value
        if lanes is not None:
            sq = value * value
            total = sq[:, :, :128]
            for b in range(1, cols // 128):
                total += sq[:, :, b * 128 : (b + 1) * 128]
            lanes[pl.ds(p, m)] = total

    def finish(c, m, i):
        p = piece(c)
        some = pl.ds(c, m)

        @pl.when(c == free)
        def _():
            early(k).wait_recv()

        @pl.when(c >= free)
        def _():
            part[k, pl.ds(p, m)] += yrecv[k, pl.ds(jnp.maximum(c - free, 0), m)].astype(F32)

        for d in range(2):

            @pl.when(at[d] > 0)
            def _():
                along(d, n - 1, i, zsend.at[d, n - 2, some], zrecv.at[d, n - 2, some]).wait_recv()
                part[k, pl.ds(p, m)] += zrecv[d, n - 2, some].astype(F32)

        fsend[some] = part[k, pl.ds(p, m)].astype(BF16)
        final(c, m, i).start()

        @pl.when(c >= free)
        def _():
            put(p, m, fsend[some].astype(F32) * factor, lanes_s)

    def deliver(c, m, i):
        final(c, m, i).wait_recv()
        some = pl.ds(c, m)

        @pl.when(c < free)
        def _():
            put(piece(c), m, (fsend[some].astype(F32) + frecv[some].astype(F32)) * factor, lanes_u)

        @pl.when(c >= free)
        def _():
            put(mate * SPLIT + c - free, m, frecv[some].astype(F32) * factor, None)

    def energy(lanes):
        return jnp.sum(lanes[...].reshape(hidden_units, 128).T, axis=0, keepdims=True)

    def free_energy(to, slot):
        return pltpu.make_async_remote_copy(
            src_ref=esu, dst_ref=eru.at[slot], send_sem=us_sem.at[0], recv_sem=ur_sem.at[0],
            device_id={"fs": to}, device_id_type=MESH,
        )

    def split_energy(other, to, slot):
        return pltpu.make_async_remote_copy(
            src_ref=ess, dst_ref=ers.at[rep, slot], send_sem=ss_sem.at[other], recv_sem=sr_sem.at[other],
            device_id={"rep": jnp.where(other == 1, mate, rep), "fs": to}, device_id_type=MESH,
        )

    blocks = 4
    brows = tokens // blocks
    units = (n - 2) * halves

    def activations(i):
        at_rows = pl.ds(pl.multiple_of(i * brows, brows), brows)
        gate = g[at_rows, :].astype(F32)
        up = u[at_rows, :].astype(F32)
        grad = dhid[at_rows, :]
        sig = jax.nn.sigmoid(gate)
        du[at_rows, :] = (grad * (gate * sig)).astype(BF16)
        dg[at_rows, :] = (grad * up * sig * (1.0 + gate * (1.0 - sig))).astype(BF16)

    def last(c, m, i):
        finish(c, m, i)

        @pl.when(i < units)
        def _():
            gather(2 + i // halves, lax.rem(i, halves))

        @pl.when((i >= units) & (i < units + blocks))
        def _():
            activations(i - units)

        @pl.when(i >= LAG)
        def _():
            deliver(c - 2 * LAG, 2, i - LAG)

        @pl.when(i == free // 2 - 1 + LAG)
        def _():
            esu[...] = energy(lanes_u)
            for t in range(1, n):
                free_energy(lax.rem(k + t, n), k).start()

    steps(0, pairs, last)
    steps(pairs, end, finish)
    ess[...] = energy(lanes_s)
    for t in range(1, n):
        split_energy(0, lax.rem(k + t, n), k).start()
    for t in range(n):
        split_energy(1, lax.rem(k + t, n), k).start()
    steps(pairs - LAG, end, deliver)

    for d in range(2):

        @pl.when(at[d] < n - 1)
        def _():
            for s in range(n):
                whole = pltpu.make_async_remote_copy(
                    src_ref=zsend.at[d, 0], dst_ref=zrecv.at[d, 0], send_sem=zs_sem.at[d, s],
                    recv_sem=zr_sem.at[d, s, 0], device_id={"fs": k + sign[d]}, device_id_type=MESH,
                )
                whole.wait_send()

    across(fsend, frecv, fs_sem.at[0], fr_sem.at[0]).wait_send()
    across(ysend, yrecv, ys_sem.at[0], yr_sem.at[0]).wait_send()

    def sent_across(j):
        @pl.when(j != k)
        def _():
            crossing(j, rep, 0, SPLIT).wait_send()

    loop(0, n, sent_across)

    def settle(some, send, recv):
        copy = across(some, some, send, recv)
        copy.wait_send()
        copy.wait_recv()

    settle(eru.at[pl.ds(0, n - 1)], us_sem.at[0], ur_sem.at[0])
    settle(ers.at[0, pl.ds(0, n - 1)], ss_sem.at[0], sr_sem.at[0])
    settle(ers.at[1], ss_sem.at[1], sr_sem.at[1])
    total = jnp.zeros((1, hidden_units), F32)
    for j in range(n):
        total += jnp.where(j == k, esu[...], eru[j])
        for r in range(2):
            total += jnp.where((j == k) & (r == rep), ess[...], ers[r, j])
    en_ref[...] = total * (1.0 / width)


def write_out(dg, du, gd, en, dg_hbm, du_hbm, gd_hbm, en_out, sem):
    copies = [
        pltpu.make_async_copy(src, dst, sem.at[i])
        for i, (src, dst) in enumerate(((dg, dg_hbm), (du, du_hbm), (gd, gd_hbm)))
    ]
    for copy in copies:
        copy.start()
    en_out[...] = en[0, :]
    for copy in copies:
        copy.wait()


def fused(n, gate_pre, up_pre, out_grad, w_down):
    tokens, units = gate_pre.shape
    width = out_grad.shape[1]
    cols = w_down.shape[1]
    rows = units // PIECES
    count = PIECES - SPLIT
    factor = float(tokens * lax.axis_size("rep") * n) ** (-0.5)
    any_spec = pl.BlockSpec(memory_space=pl.ANY)
    vmem_spec = pl.BlockSpec(memory_space=pltpu.VMEM)
    dma = pltpu.SemaphoreType.DMA
    d_gate, d_up, grad, energy = pl.pallas_call(
        functools.partial(kernel, n, factor, width),
        out_shape=(
            pltpu.VMEM((tokens, units), BF16),
            pltpu.VMEM((tokens, units), BF16),
            pltpu.VMEM((PIECES, rows, cols), F32),
            pltpu.VMEM((1, units), F32),
        ),
        in_specs=[any_spec] * 4,
        out_specs=(vmem_spec,) * 4,
        scratch_shapes=[
            pltpu.VMEM((tokens, units), BF16),
            pltpu.VMEM((tokens, units), BF16),
            pltpu.VMEM((n, tokens, cols), BF16),
            pltpu.VMEM((n, PIECES, rows, cols), BF16),
            pltpu.VMEM((units, tokens), BF16),
            pltpu.VMEM((n, PIECES, rows, cols), F32),
            pltpu.VMEM((tokens, units), F32),
            pltpu.VMEM((2, n - 1, count, rows, cols), BF16),
            pltpu.VMEM((2, n - 1, count, rows, cols), BF16),
            pltpu.VMEM((n, SPLIT, rows, cols), BF16),
            pltpu.VMEM((n, SPLIT, rows, cols), BF16),
            pltpu.VMEM((count, rows, cols), BF16),
            pltpu.VMEM((count, rows, cols), BF16),
            pltpu.VMEM((PIECES, rows, 128), F32),
            pltpu.VMEM((PIECES, rows, 128), F32),
            pltpu.VMEM((1, units), F32),
            pltpu.VMEM((n, 1, units), F32),
            pltpu.VMEM((1, units), F32),
            pltpu.VMEM((2, n, 1, units), F32),
            dma((1 + 2 * LOADS,)),
            dma((n,)),
            dma((2, n)),
            dma((2, n, (count + 1) // 2)),
            dma((n,)),
            dma((n,)),
            dma((1,)),
            dma((n,)),
            dma((1,)),
            dma(((count + 1) // 2,)),
            dma((1,)),
            dma((1,)),
            dma((2,)),
            dma((2,)),
        ],
        compiler_params=pltpu.CompilerParams(
            collective_id=0, has_side_effects=True, vmem_limit_bytes=VMEM_LIMIT
        ),
    )(gate_pre, up_pre, out_grad, w_down.reshape(PIECES, rows, cols))
    return pl.pallas_call(
        write_out,
        out_shape=(
            jax.ShapeDtypeStruct((tokens, units), BF16),
            jax.ShapeDtypeStruct((tokens, units), BF16),
            jax.ShapeDtypeStruct((units, cols), F32),
            jax.ShapeDtypeStruct((units,), F32),
        ),
        in_specs=[vmem_spec] * 4,
        out_specs=(any_spec, any_spec, any_spec, vmem_spec),
        scratch_shapes=[dma((3,))],
        compiler_params=pltpu.CompilerParams(vmem_limit_bytes=4 * 1024 * 1024),
    )(d_gate, d_up, grad.reshape(units, cols), energy)


def solution(mesh):
    reps, n = mesh.shape["rep"], mesh.shape["fs"]

    def local(gate_pre, up_pre, out_grad, w_down):
        units, cols = w_down.shape
        fits = reps == 2 and 2 <= n <= 4 and cols % 128 == 0 and units % (PIECES * 16) == 0 and units % 128 == 0
        if fits and gate_pre.shape[0] % 1024 == 0:
            return fused(n, gate_pre, up_pre, out_grad, w_down)
        return plain(gate_pre, up_pre, out_grad, w_down)

    placed = (P(("rep", "fs"), "tp"), P(("rep", "fs"), "tp"), P(("rep", "fs"), None), P("tp", "fs"))
    return jax.shard_map(
        local,
        mesh=mesh,
        in_specs=placed,
        out_specs=(P(("rep", "fs"), "tp"), P(("rep", "fs"), "tp"), P("tp", "fs"), P("tp")),
        check_vma=False,
    )
```

```python
import functools

import jax
import jax.numpy as jnp
from jax import lax
from jax.experimental import pallas as pl
from jax.experimental.pallas import tpu as pltpu
from jax.sharding import PartitionSpec as P

MESH = pl.DeviceIdType.MESH
F32 = jnp.float32
BF16 = jnp.bfloat16
PIECES = 16
SPLIT = 5
GROUP = 2
LAG = 2
NEAR = 2
LOADS = 4
BEFORE = 1
VMEM_LIMIT = 52 * 1024 * 1024


def plain(gate_pre, up_pre, out_grad, w_down):
    gate_f = gate_pre.astype(F32)
    up_f = up_pre.astype(F32)
    sig = jax.nn.sigmoid(gate_f)
    act = gate_f * sig
    hidden = (act * up_f).astype(BF16)
    tokens_all = out_grad.shape[0] * lax.axis_size("rep") * lax.axis_size("fs")
    factor = float(tokens_all) ** (-0.5)
    weight_whole = lax.all_gather(w_down, "fs", axis=1, tiled=True)
    dhid = lax.dot_general(out_grad, weight_whole, (((1,), (1,)), ((), ())), preferred_element_type=F32)
    d_up = (dhid * act).astype(BF16)
    d_gate = (dhid * up_f * sig * (1.0 + gate_f * (1.0 - sig))).astype(BF16)
    shard = lax.psum_scatter(
        lax.dot_general(out_grad, hidden, (((0,), (0,)), ((), ())), preferred_element_type=F32),
        "fs",
        scatter_dimension=0,
        tiled=True,
    )
    shard = lax.psum(shard, "rep")
    grad_down = shard.T * factor
    energy = lax.psum(jnp.sum(grad_down * grad_down, axis=1), "fs") / out_grad.shape[1]
    return (d_gate, d_up, grad_down, energy)


def kernel(
    n, factor, width,
    g_hbm, u_hbm, og_hbm, w_hbm,
    dg, du, gd, en_ref,
    g, u, og, w, hid, part, dhid, zsend, zrecv, ysend, yrecv, fsend, frecv,
    lanes_u, lanes_s, esu, eru, ess, ers,
    in_sem, og_sem, zs_sem, zr_sem, as_sem, ar_sem, ys_sem, yr_sem, fs_sem, fr_sem,
    us_sem, ur_sem, ss_sem, sr_sem,
):
    rep = lax.axis_index("rep")
    k = lax.axis_index("fs")
    mate = 1 - rep
    cols = w.shape[3]
    rows = w.shape[2]
    hidden_units = g.shape[1]
    tokens = g.shape[0]
    count = PIECES - SPLIT
    free = PIECES - 2 * SPLIT
    pairs = count // GROUP
    chunk = tokens // LOADS

    def piece(c):
        return c + jnp.where(c < free, 2 * SPLIT, rep * SPLIT - free)

    def loop(lo, hi, body):
        lax.fori_loop(lo, hi, lambda i, x: (body(i), x)[1], 0)

    def steps(lo, hi, body):
        loop(lo, min(hi, pairs), lambda i: body(GROUP * i, GROUP, i))
        if hi > pairs:
            body(k * 0 + GROUP * pairs, count % GROUP, k * 0 + pairs)

    end = -(-count // GROUP)
    low = jnp.minimum(k, n - 1 - k)

    def chosen(i):
        far = jnp.where(i < n - 1 - low, n - 1 - i, jnp.where(i < n - 1, i - (n - 1 - low), low))
        return jnp.where(2 * k >= n, n - 1 - far, far)

    def rows_at(i):
        return pl.ds(pl.multiple_of(i * chunk, chunk), chunk)

    wide = -(-2 * SPLIT * rows // 128) * 128
    spans = ((0, wide), (wide, hidden_units - wide)) if wide < hidden_units else ((0, wide),)

    def in_gate(h, i):
        at = (rows_at(i), pl.ds(*spans[h]))
        return pltpu.make_async_copy(g_hbm.at[at], g.at[at], in_sem.at[1 + 2 * LOADS * h + i])

    def in_up(h, i):
        at = (rows_at(i), pl.ds(*spans[h]))
        return pltpu.make_async_copy(u_hbm.at[at], u.at[at], in_sem.at[1 + 2 * LOADS * h + LOADS + i])

    def in_og(j):
        part_of = pl.ds(pl.multiple_of(j * cols, cols), cols)
        return pltpu.make_async_copy(og_hbm.at[:, part_of], og.at[j], og_sem.at[j])

    at = (k, n - 1 - k)
    sign = (1, -1)

    barrier = pltpu.get_barrier_semaphore()
    for d in range(2):

        @pl.when(at[d] < n - 1)
        def _():
            pl.semaphore_signal(barrier, inc=1, device_id={"fs": k + sign[d]}, device_id_type=MESH)

    pl.semaphore_signal(barrier, inc=1, device_id={"rep": mate}, device_id_type=MESH)
    in_w = pltpu.make_async_copy(w_hbm, w.at[k], in_sem.at[0])
    in_w.start()

    def load(h, i):
        in_gate(h, i).start()
        in_up(h, i).start()

    loop(0, LOADS, functools.partial(load, 0))
    in_og(chosen(0)).start()
    for h in range(1, len(spans)):
        loop(0, LOADS, functools.partial(load, h))
    loop(1, n, lambda i: in_og(chosen(i)).start())
    def along(d, s, i, src, dst):
        return pltpu.make_async_remote_copy(
            src_ref=src, dst_ref=dst, send_sem=zs_sem.at[d], recv_sem=zr_sem.at[d, s % 3, i],
            device_id={"fs": k + sign[d]}, device_id_type=MESH,
        )

    def across(src, dst, send, recv):
        return pltpu.make_async_remote_copy(
            src_ref=src, dst_ref=dst, send_sem=send, recv_sem=recv,
            device_id={"rep": mate}, device_id_type=MESH,
        )

    def early(j):
        return across(ysend.at[j], yrecv.at[j], ys_sem.at[0], yr_sem.at[j])

    def final(c, m, i):
        return across(fsend.at[pl.ds(c, m)], frecv.at[pl.ds(c, m)], fs_sem.at[0], fr_sem.at[i])

    def crossing(j, owner, start, m):
        block = w.at[j, pl.ds(owner * SPLIT + start, m)]
        return across(block, block, as_sem.at[0], ar_sem.at[j])

    def make_hidden(h, i):
        in_gate(h, i).wait()
        in_up(h, i).wait()
        start, width = spans[h]
        at = (rows_at(i), pl.ds(start, width))
        gate = g[at].astype(F32)
        act = gate * jax.nn.sigmoid(gate)
        hid[pl.ds(start, width), rows_at(i)] = (act * u[at].astype(F32)).astype(BF16).T

    loop(0, BEFORE, functools.partial(make_hidden, 0))
    pl.semaphore_wait(barrier, 1 + (k > 0).astype(jnp.int32) + (k < n - 1).astype(jnp.int32))
    in_w.wait()

    def first(c, m, i):
        for d in range(2):

            @pl.when(at[d] < n - 1)
            def _():
                block = w.at[k, pl.ds(piece(c), m)]
                along(d, 0, i, block, block).start()

    steps(0, end, first)
    loop(BEFORE, LOADS, functools.partial(make_hidden, 0))

    def product(j, start, pieces):
        some = hid[pl.ds(pl.multiple_of(start * rows, rows), pieces * rows), :]
        return jnp.dot(some, og[j], preferred_element_type=F32).reshape(pieces, rows, cols)

    def make_early(i):
        j = chosen(i)
        in_og(j).wait()
        ysend[j] = product(j, mate * SPLIT, SPLIT).astype(BF16)
        early(j).start()

    def make_part(j):
        part[j, pl.ds(2 * SPLIT, free)] = product(j, 2 * SPLIT, free)
        part[j, pl.ds(rep * SPLIT, SPLIT)] = product(j, rep * SPLIT, SPLIT)

    loop(0, n, make_early)
    for h in range(1, len(spans)):
        loop(0, LOADS, functools.partial(make_hidden, h))
    loop(0, n, make_part)
    lanes_u[...] = jnp.zeros_like(lanes_u)
    lanes_s[...] = jnp.zeros_like(lanes_s)

    def multiply(j, at_rows):
        return lax.dot_general(
            og[j, at_rows, :], w[j].reshape(hidden_units, cols), (((1,), (1,)), ((), ())),
            preferred_element_type=F32,
        )

    def own(i):
        at_rows = pl.ds(pl.multiple_of(i * 256, 256), 256)
        dhid[at_rows, :] = multiply(k, at_rows)

    loop(0, tokens // 256, own)

    def pass_on(s, c, m, i):
        p = piece(c)
        for d in range(2):
            place = at[d]
            some = pl.ds(c, m)

            @pl.when(place > 0)
            def _():
                along(d, s - 1, i, zsend.at[d, 0, some], zrecv.at[d, 0, some]).wait_recv()

            @pl.when(s <= place)
            def _():
                j = k - sign[d] * s
                block = w.at[j, pl.ds(p, m)]

                @pl.when(place < n - 1)
                def _():
                    along(d, s, i, block, block).start()

                @pl.when(c >= free)
                def _():
                    crossing(j, rep, c - free, m).start()

            @pl.when(s > place)
            def _():
                j = k + sign[d] * (n - s)

                @pl.when(c == free)
                def _():
                    early(j).wait_recv()

                @pl.when(c >= free)
                def _():
                    part[j, pl.ds(p, m)] += yrecv[j, pl.ds(jnp.maximum(c - free, 0), m)].astype(F32)

                if s > 1:

                    @pl.when(place > 0)
                    def _():
                        part[j, pl.ds(p, m)] += zrecv[d, s - 2, some].astype(F32)

                zsend[d, s - 1, some] = part[j, pl.ds(p, m)].astype(BF16)
                along(d, s, i, zsend.at[d, s - 1, some], zrecv.at[d, s - 1, some]).start()

    def gathered(j):
        crossing(j, mate, 0, SPLIT).wait_recv()

    halves = 2
    half = tokens // halves

    def gather(far, part_of):
        at_rows = pl.ds(pl.multiple_of(part_of * half, half), half)
        for d in range(2):

            @pl.when(at[d] >= far)
            def _():
                j = k - sign[d] * far

                @pl.when(part_of == 0)
                def _():
                    gathered(j)

                dhid[at_rows, :] += multiply(j, at_rows)

    for s in range(1, n - 1):
        steps(0, end, functools.partial(pass_on, s))
    steps(0, NEAR, functools.partial(pass_on, n - 1))
    loop(0, halves, functools.partial(gather, 1))
    steps(NEAR, end, functools.partial(pass_on, n - 1))

    def put(p, m, value, lanes):
        gd[pl.ds(p, m)] = value
        if lanes is not None:
            sq = value * value
            total = sq[:, :, :128]
            for b in range(1, cols // 128):
                total += sq[:, :, b * 128 : (b + 1) * 128]
            lanes[pl.ds(p, m)] = total

    def finish(c, m, i):
        p = piece(c)
        some = pl.ds(c, m)

        @pl.when(c == free)
        def _():
            early(k).wait_recv()

        @pl.when(c >= free)
        def _():
            part[k, pl.ds(p, m)] += yrecv[k, pl.ds(jnp.maximum(c - free, 0), m)].astype(F32)

        for d in range(2):

            @pl.when(at[d] > 0)
            def _():
                along(d, n - 1, i, zsend.at[d, n - 2, some], zrecv.at[d, n - 2, some]).wait_recv()
                part[k, pl.ds(p, m)] += zrecv[d, n - 2, some].astype(F32)

        fsend[some] = part[k, pl.ds(p, m)].astype(BF16)
        final(c, m, i).start()

        @pl.when(c >= free)
        def _():
            put(p, m, fsend[some].astype(F32) * factor, lanes_s)

    def deliver(c, m, i):
        final(c, m, i).wait_recv()
        some = pl.ds(c, m)

        @pl.when(c < free)
        def _():
            put(piece(c), m, (fsend[some].astype(F32) + frecv[some].astype(F32)) * factor, lanes_u)

        @pl.when(c >= free)
        def _():
            put(mate * SPLIT + c - free, m, frecv[some].astype(F32) * factor, None)

    def energy(lanes):
        return jnp.sum(lanes[...].reshape(hidden_units, 128).T, axis=0, keepdims=True)

    def free_energy(to, slot):
        return pltpu.make_async_remote_copy(
            src_ref=esu, dst_ref=eru.at[slot], send_sem=us_sem.at[0], recv_sem=ur_sem.at[0],
            device_id={"fs": to}, device_id_type=MESH,
        )

    def split_energy(other, to, slot):
        return pltpu.make_async_remote_copy(
            src_ref=ess, dst_ref=ers.at[rep, slot], send_sem=ss_sem.at[other], recv_sem=sr_sem.at[other],
            device_id={"rep": jnp.where(other == 1, mate, rep), "fs": to}, device_id_type=MESH,
        )

    blocks = 4
    brows = tokens // blocks
    units = (n - 2) * halves
    each = -(-(units + blocks) // (end - 1))

    def activations(i):
        at_rows = pl.ds(pl.multiple_of(i * brows, brows), brows)
        gate = g[at_rows, :].astype(F32)
        up = u[at_rows, :].astype(F32)
        grad = dhid[at_rows, :]
        sig = jax.nn.sigmoid(gate)
        du[at_rows, :] = (grad * (gate * sig)).astype(BF16)
        dg[at_rows, :] = (grad * up * sig * (1.0 + gate * (1.0 - sig))).astype(BF16)

    def last(c, m, i):
        finish(c, m, i)

        for a in range(each):
            q = i * each + a

            @pl.when(q < units)
            def _():
                gather(2 + q // halves, lax.rem(q, halves))

            @pl.when((q >= units) & (q < units + blocks))
            def _():
                activations(q - units)

        @pl.when(i >= LAG)
        def _():
            deliver(c - GROUP * LAG, GROUP, i - LAG)

        @pl.when(i == free // GROUP - 1 + LAG)
        def _():
            esu[...] = energy(lanes_u)
            for t in range(1, n):
                free_energy(lax.rem(k + t, n), k).start()

    steps(0, end - 1, last)
    steps(end - 1, end, finish)
    ess[...] = energy(lanes_s)
    for t in range(1, n):
        split_energy(0, lax.rem(k + t, n), k).start()
    for t in range(n):
        split_energy(1, lax.rem(k + t, n), k).start()
    steps(end - 1 - LAG, end, deliver)

    for d in range(2):

        @pl.when(at[d] < n - 1)
        def _():
            along(d, 0, 0, w.at[:, pl.ds(0, count)], w.at[:, pl.ds(0, count)]).wait_send()

    across(fsend, frecv, fs_sem.at[0], fr_sem.at[0]).wait_send()
    across(ysend, yrecv, ys_sem.at[0], yr_sem.at[0]).wait_send()

    crossed = w.at[pl.ds(0, n - 1), pl.ds(0, SPLIT)]
    across(crossed, crossed, as_sem.at[0], ar_sem.at[0]).wait_send()

    def settle(some, send, recv):
        copy = across(some, some, send, recv)
        copy.wait_send()
        copy.wait_recv()

    settle(eru.at[pl.ds(0, n - 1)], us_sem.at[0], ur_sem.at[0])
    settle(ers.at[0, pl.ds(0, n - 1)], ss_sem.at[0], sr_sem.at[0])
    settle(ers.at[1], ss_sem.at[1], sr_sem.at[1])
    total = jnp.zeros((1, hidden_units), F32)
    for j in range(n):
        total += jnp.where(j == k, esu[...], eru[j])
        for r in range(2):
            total += jnp.where((j == k) & (r == rep), ess[...], ers[r, j])
    en_ref[...] = total * (1.0 / width)


def write_out(dg, du, gd, en, dg_hbm, du_hbm, gd_hbm, en_hbm, flat, sem):
    def copy_of(i, src, dst):
        return pltpu.make_async_copy(src, dst, sem.at[i])

    copies = [copy_of(0, dg, dg_hbm), copy_of(1, du, du_hbm), copy_of(2, gd, gd_hbm)]
    for copy in copies:
        copy.start()
    flat[...] = en[0, :]
    copies.append(copy_of(3, flat, en_hbm))
    copies[3].start()
    for copy in copies:
        copy.wait()


def fused(n, gate_pre, up_pre, out_grad, w_down):
    tokens, units = gate_pre.shape
    width = out_grad.shape[1]
    cols = w_down.shape[1]
    rows = units // PIECES
    count = PIECES - SPLIT
    factor = float(tokens * lax.axis_size("rep") * n) ** (-0.5)
    any_spec = pl.BlockSpec(memory_space=pl.ANY)
    vmem_spec = pl.BlockSpec(memory_space=pltpu.VMEM)
    dma = pltpu.SemaphoreType.DMA
    d_gate, d_up, grad, energy = pl.pallas_call(
        functools.partial(kernel, n, factor, width),
        out_shape=(
            pltpu.VMEM((tokens, units), BF16),
            pltpu.VMEM((tokens, units), BF16),
            pltpu.VMEM((PIECES, rows, cols), F32),
            pltpu.VMEM((1, units), F32),
        ),
        in_specs=[any_spec] * 4,
        out_specs=(vmem_spec,) * 4,
        scratch_shapes=[
            pltpu.VMEM((tokens, units), BF16),
            pltpu.VMEM((tokens, units), BF16),
            pltpu.VMEM((n, tokens, cols), BF16),
            pltpu.VMEM((n, PIECES, rows, cols), BF16),
            pltpu.VMEM((units, tokens), BF16),
            pltpu.VMEM((n, PIECES, rows, cols), F32),
            pltpu.VMEM((tokens, units), F32),
            pltpu.VMEM((2, n - 1, count, rows, cols), BF16),
            pltpu.VMEM((2, n - 1, count, rows, cols), BF16),
            pltpu.VMEM((n, SPLIT, rows, cols), BF16),
            pltpu.VMEM((n, SPLIT, rows, cols), BF16),
            pltpu.VMEM((count, rows, cols), BF16),
            pltpu.VMEM((count, rows, cols), BF16),
            pltpu.VMEM((PIECES, rows, 128), F32),
            pltpu.VMEM((PIECES, rows, 128), F32),
            pltpu.VMEM((1, units), F32),
            pltpu.VMEM((n, 1, units), F32),
            pltpu.VMEM((1, units), F32),
            pltpu.VMEM((2, n, 1, units), F32),
            dma((1 + 4 * LOADS,)),
            dma((n,)),
            dma((2,)),
            dma((2, min(n, 3), -(-count // GROUP))),
            dma((1,)),
            dma((n,)),
            dma((1,)),
            dma((n,)),
            dma((1,)),
            dma((-(-count // GROUP),)),
            dma((1,)),
            dma((1,)),
            dma((2,)),
            dma((2,)),
        ],
        compiler_params=pltpu.CompilerParams(
            collective_id=0, has_side_effects=True, vmem_limit_bytes=VMEM_LIMIT
        ),
    )(gate_pre, up_pre, out_grad, w_down.reshape(PIECES, rows, cols))
    return pl.pallas_call(
        write_out,
        out_shape=(
            jax.ShapeDtypeStruct((tokens, units), BF16),
            jax.ShapeDtypeStruct((tokens, units), BF16),
            jax.ShapeDtypeStruct((units, cols), F32),
            jax.ShapeDtypeStruct((units,), F32),
        ),
        in_specs=[vmem_spec] * 4,
        out_specs=(any_spec,) * 4,
        scratch_shapes=[pltpu.VMEM((units,), F32), dma((4,))],
        compiler_params=pltpu.CompilerParams(vmem_limit_bytes=4 * 1024 * 1024),
    )(d_gate, d_up, grad.reshape(units, cols), energy)


def solution(mesh):
    reps, n = mesh.shape["rep"], mesh.shape["fs"]

    def local(gate_pre, up_pre, out_grad, w_down):
        units, cols = w_down.shape
        fits = reps == 2 and 2 <= n <= 4 and cols % 128 == 0 and units % (PIECES * 16) == 0 and units % 128 == 0
        if fits and gate_pre.shape[0] % 1024 == 0:
            return fused(n, gate_pre, up_pre, out_grad, w_down)
        return plain(gate_pre, up_pre, out_grad, w_down)

    placed = (P(("rep", "fs"), "tp"), P(("rep", "fs"), "tp"), P(("rep", "fs"), None), P("tp", "fs"))
    return jax.shard_map(
        local,
        mesh=mesh,
        in_specs=placed,
        out_specs=(P(("rep", "fs"), "tp"), P(("rep", "fs"), "tp"), P("tp", "fs"), P("tp")),
        check_vma=False,
    )
```

```python
import functools

import jax
import jax.numpy as jnp
from jax import lax
from jax.experimental import pallas as pl
from jax.experimental.pallas import tpu as pltpu
from jax.sharding import PartitionSpec as P

MESH = pl.DeviceIdType.MESH
F32 = jnp.float32
BF16 = jnp.bfloat16
PIECES = 16
SPLIT = 5
GROUP = 2
FIRST = 2
FROM = 1
LOADS = 4
BEFORE = 0
VMEM_LIMIT = 52 * 1024 * 1024


def plain(gate_pre, up_pre, out_grad, w_down):
    gate_f = gate_pre.astype(F32)
    up_f = up_pre.astype(F32)
    sig = jax.nn.sigmoid(gate_f)
    act = gate_f * sig
    hidden = (act * up_f).astype(BF16)
    tokens_all = out_grad.shape[0] * lax.axis_size("rep") * lax.axis_size("fs")
    factor = float(tokens_all) ** (-0.5)
    weight_whole = lax.all_gather(w_down, "fs", axis=1, tiled=True)
    dhid = lax.dot_general(out_grad, weight_whole, (((1,), (1,)), ((), ())), preferred_element_type=F32)
    d_up = (dhid * act).astype(BF16)
    d_gate = (dhid * up_f * sig * (1.0 + gate_f * (1.0 - sig))).astype(BF16)
    shard = lax.psum_scatter(
        lax.dot_general(out_grad, hidden, (((0,), (0,)), ((), ())), preferred_element_type=F32),
        "fs",
        scatter_dimension=0,
        tiled=True,
    )
    shard = lax.psum(shard, "rep")
    grad_down = shard.T * factor
    energy = lax.psum(jnp.sum(grad_down * grad_down, axis=1), "fs") / out_grad.shape[1]
    return (d_gate, d_up, grad_down, energy)


def kernel(
    n, factor, width,
    g_hbm, u_hbm, og_hbm, w_hbm,
    dg, du, gd, en_ref,
    g, u, og, w, hid, part, dhid, zsend, zrecv, ysend, yrecv, fsend, frecv,
    lanes_u, lanes_s, esu, eru, ess, ers,
    in_sem, og_sem, zs_sem, zr_sem, zx_sem, as_sem, ar_sem, ys_sem, yr_sem, fs_sem, fr_sem,
    us_sem, ur_sem, ss_sem, sr_sem,
):
    rep = lax.axis_index("rep")
    k = lax.axis_index("fs")
    mate = 1 - rep
    cols = w.shape[3]
    rows = w.shape[2]
    hidden_units = g.shape[1]
    tokens = g.shape[0]
    count = PIECES - SPLIT
    free = PIECES - 2 * SPLIT
    pairs = count // GROUP
    chunk = tokens // LOADS

    def piece(c):
        return c + jnp.where(c < free, 2 * SPLIT, rep * SPLIT - free)

    def loop(lo, hi, body):
        lax.fori_loop(lo, hi, lambda i, x: (body(i), x)[1], 0)

    def steps(lo, hi, body):
        loop(lo, min(hi, pairs), lambda i: body(GROUP * i, GROUP, i))
        if hi > pairs:
            body(k * 0 + GROUP * pairs, count % GROUP, k * 0 + pairs)

    end = -(-count // GROUP)
    late = free // GROUP - 1
    low = jnp.minimum(k, n - 1 - k)

    def chosen(i):
        far = jnp.where(i < n - 1 - low, n - 1 - i, jnp.where(i < n - 1, i - (n - 1 - low), low))
        return jnp.where(2 * k >= n, n - 1 - far, far)

    def rows_at(i):
        return pl.ds(pl.multiple_of(i * chunk, chunk), chunk)

    wide = -(-2 * SPLIT * rows // 128) * 128
    spans = ((0, wide), (wide, hidden_units - wide)) if wide < hidden_units else ((0, wide),)

    def in_gate(h, i):
        at = (rows_at(i) if h == 0 else pl.ds(0, tokens), pl.ds(*spans[h]))
        return pltpu.make_async_copy(g_hbm.at[at], g.at[at], in_sem.at[4 + 2 * i if h == 0 else 2])

    def in_up(h, i):
        at = (rows_at(i) if h == 0 else pl.ds(0, tokens), pl.ds(*spans[h]))
        return pltpu.make_async_copy(u_hbm.at[at], u.at[at], in_sem.at[5 + 2 * i if h == 0 else 3])

    def in_og(j):
        part_of = pl.ds(pl.multiple_of(j * cols, cols), cols)
        return pltpu.make_async_copy(og_hbm.at[:, part_of], og.at[j], og_sem.at[j])

    at = (k, n - 1 - k)
    sign = (1, -1)

    barrier = pltpu.get_barrier_semaphore()
    for d in range(2):

        @pl.when(at[d] < n - 1)
        def _():
            pl.semaphore_signal(barrier, inc=1, device_id={"fs": k + sign[d]}, device_id_type=MESH)

    pl.semaphore_signal(barrier, inc=1, device_id={"rep": mate}, device_id_type=MESH)
    in_w = [
        pltpu.make_async_copy(w_hbm.at[some], w.at[k, some], in_sem.at[i])
        for i, some in enumerate((pl.ds(2 * SPLIT, free), pl.ds(0, 2 * SPLIT)))
    ]
    for copy in in_w:
        copy.start()

    def load(h, i):
        in_gate(h, i).start()
        in_up(h, i).start()

    loop(0, LOADS, functools.partial(load, 0))
    in_og(chosen(0)).start()
    for h in range(1, len(spans)):
        load(h, 0)
    loop(1, n, lambda i: in_og(chosen(i)).start())
    def along(d, s, i, src, dst, kind=0):
        return pltpu.make_async_remote_copy(
            src_ref=src, dst_ref=dst, send_sem=zs_sem.at[d, kind], recv_sem=zr_sem.at[d, lax.rem(s * end + i, 2 * end + 1)],
            device_id={"fs": k + sign[d]}, device_id_type=MESH,
        )

    def block_of(j, p, m, i):
        brief = (i == 0) & (rep == 1) & (j == n - 1)

        def each_size(act):
            @pl.when(brief)
            def _():
                act(w.at[j, pl.ds(p, m - 1)])

            @pl.when(jnp.logical_not(brief))
            def _():
                act(w.at[j, pl.ds(p, m)])

        return each_size

    def spread(pieces):
        blocks = next(b for b in range(1, n + 1) if pieces % b == 0 and pieces // b <= PIECES)
        return w.at[pl.ds(0, blocks), pl.ds(0, pieces // blocks)]

    def send_block(d, s, i, j, p, m):
        if m > 1:
            block_of(j, p, m, i)(lambda block: along(d, s, i, block, block).start())
        else:
            block = w.at[j, pl.ds(p, m)]
            along(d, s, i, block, block).start()

    def take_block(d, s, i, j, p, m):
        if m > 1:
            block_of(j, p, m, i)(lambda block: along(d, s, i, block, block).wait_recv())
        else:
            block = w.at[j, pl.ds(p, m)]
            along(d, s, i, block, block).wait_recv()

    def deferred(d):
        block = w.at[k, pl.ds(2 * SPLIT + late * GROUP, GROUP)]
        return pltpu.make_async_remote_copy(
            src_ref=block, dst_ref=block, send_sem=zs_sem.at[d, 0], recv_sem=zx_sem.at[d],
            device_id={"fs": k + sign[d]}, device_id_type=MESH,
        )

    def across(src, dst, send, recv):
        return pltpu.make_async_remote_copy(
            src_ref=src, dst_ref=dst, send_sem=send, recv_sem=recv,
            device_id={"rep": mate}, device_id_type=MESH,
        )

    def early(j):
        return across(ysend.at[j], yrecv.at[j], ys_sem.at[0], yr_sem.at[j])

    def final(c, m, i):
        return across(fsend.at[pl.ds(c, m)], frecv.at[pl.ds(c, m)], fs_sem.at[0], fr_sem.at[i])

    def crossing(j, owner, start, m):
        block = w.at[j, pl.ds(owner * SPLIT + start, m)]
        return across(block, block, as_sem.at[0], ar_sem.at[j])

    def loaded(h, i):
        in_gate(h, i).wait()
        in_up(h, i).wait()

    def make_hidden(h, i):
        if h == 0:
            loaded(h, i)
        start, width = spans[h]
        at = (rows_at(i), pl.ds(start, width))
        gate = g[at].astype(F32)
        act = gate * jax.nn.sigmoid(gate)
        hid[pl.ds(start, width), rows_at(i)] = (act * u[at].astype(F32)).astype(BF16).T

    loop(0, BEFORE, functools.partial(make_hidden, 0))
    pl.semaphore_wait(barrier, 1 + (k > 0).astype(jnp.int32) + (k < n - 1).astype(jnp.int32))
    in_w[0].wait()

    def first(c, m, i):
        for d in range(2):

            @pl.when((at[d] < n - 2) | ((at[d] == n - 2) & (i != late)))
            def _():
                send_block(d, 0, i, k, piece(c), m)

    steps(0, free // GROUP, first)
    in_w[1].wait()
    steps(free // GROUP, end, first)
    loop(BEFORE, LOADS, functools.partial(make_hidden, 0))

    def product(j, start, pieces):
        some = hid[pl.ds(pl.multiple_of(start * rows, rows), pieces * rows), :]
        return jnp.dot(some, og[j], preferred_element_type=F32).reshape(pieces, rows, cols)

    def make_early(i):
        j = chosen(i)
        in_og(j).wait()
        ysend[j] = product(j, mate * SPLIT, SPLIT).astype(BF16)
        early(j).start()

    def make_part(j):
        part[j, pl.ds(2 * SPLIT, free)] = product(j, 2 * SPLIT, free)
        part[j, pl.ds(rep * SPLIT, SPLIT)] = product(j, rep * SPLIT, SPLIT)

    loop(0, n, make_early)
    for h in range(1, len(spans)):
        loaded(h, 0)
        loop(0, LOADS, functools.partial(make_hidden, h))
    loop(0, n, make_part)
    lanes_u[...] = jnp.zeros_like(lanes_u)
    lanes_s[...] = jnp.zeros_like(lanes_s)

    def multiply(j, at_rows):
        return lax.dot_general(
            og[j, at_rows, :], w[j].reshape(hidden_units, cols), (((1,), (1,)), ((), ())),
            preferred_element_type=F32,
        )

    def own(i):
        at_rows = pl.ds(pl.multiple_of(i * 256, 256), 256)
        dhid[at_rows, :] = multiply(k, at_rows)

    loop(0, tokens // 256, own)

    def pass_on(s, c, m, i):
        p = piece(c)
        for d in range(2):
            place = at[d]
            some = pl.ds(c, m)

            came = place > 0
            if s == 1:
                came &= (place < n - 1) | (i != late)

            @pl.when(came & (s > place))
            def _():
                along(d, s - 1, i, zsend.at[d, 0, some], zrecv.at[d, 0, some]).wait_recv()

            @pl.when(s <= place)
            def _():
                j = k - sign[d] * s

                @pl.when(came)
                def _():
                    take_block(d, s - 1, i, j, p, m)

                @pl.when(place < n - 1)
                def _():
                    send_block(d, s, i, j, p, m)

                @pl.when(c >= free)
                def _():
                    crossing(j, rep, c - free, m).start()

                @pl.when((i == 0) & (rep == 0) & (j == n - 1))
                def _():
                    extra = w.at[j, pl.ds(2 * SPLIT + GROUP - 1, 1)]
                    across(extra, extra, as_sem.at[0], ar_sem.at[j]).start()

            @pl.when(s > place)
            def _():
                j = k + sign[d] * (n - s)

                @pl.when(c == free)
                def _():
                    early(j).wait_recv()

                @pl.when(c >= free)
                def _():
                    part[j, pl.ds(p, m)] += yrecv[j, pl.ds(jnp.maximum(c - free, 0), m)].astype(F32)

                if s > 1:

                    @pl.when(place > 0)
                    def _():
                        part[j, pl.ds(p, m)] += zrecv[d, s - 2, some].astype(F32)

                zsend[d, s - 1, some] = part[j, pl.ds(p, m)].astype(BF16)
                along(d, s, i, zsend.at[d, s - 1, some], zrecv.at[d, s - 1, some], 1).start()

    def gathered(j):
        for r in range(2):

            @pl.when(((rep == 1) & (j == n - 1)) == (r == 1))
            def _():
                some = w.at[j, pl.ds(0, SPLIT + r)]
                across(some, some, as_sem.at[0], ar_sem.at[j]).wait_recv()

    halves = 2
    half = tokens // halves

    def gather(far, part_of, ends=None):
        at_rows = pl.ds(pl.multiple_of(part_of * half, half), half)
        for d in range(2):
            here = at[d] >= far
            if ends is not None:
                here &= (at[d] == n - 1) == ends

            @pl.when(here)
            def _():
                j = k - sign[d] * far

                @pl.when(part_of == 0)
                def _():
                    gathered(j)
                    if ends:
                        deferred(d).wait_recv()

                dhid[at_rows, :] += multiply(j, at_rows)

    for s in range(1, n - 1):
        steps(0, end, functools.partial(pass_on, s))
    steps(0, end, functools.partial(pass_on, n - 1))
    for d in range(2):

        @pl.when(at[d] == n - 2)
        def _():
            deferred(d).start()

    def put(p, m, value, lanes):
        gd[pl.ds(p, m)] = value
        if lanes is not None:
            sq = value * value
            total = sq[:, :, :128]
            for b in range(1, cols // 128):
                total += sq[:, :, b * 128 : (b + 1) * 128]
            lanes[pl.ds(p, m)] = total

    def finish(c, m, i):
        p = piece(c)
        some = pl.ds(c, m)

        @pl.when(c == free)
        def _():
            early(k).wait_recv()

        @pl.when(c >= free)
        def _():
            part[k, pl.ds(p, m)] += yrecv[k, pl.ds(jnp.maximum(c - free, 0), m)].astype(F32)

        for d in range(2):

            @pl.when(at[d] > 0)
            def _():
                along(d, n - 1, i, zsend.at[d, n - 2, some], zrecv.at[d, n - 2, some]).wait_recv()
                part[k, pl.ds(p, m)] += zrecv[d, n - 2, some].astype(F32)

        fsend[some] = part[k, pl.ds(p, m)].astype(BF16)
        final(c, m, i).start()

        @pl.when(c >= free)
        def _():
            put(p, m, fsend[some].astype(F32) * factor, lanes_s)

    def deliver(c, m, i):
        final(c, m, i).wait_recv()
        some = pl.ds(c, m)

        @pl.when(c < free)
        def _():
            put(piece(c), m, (fsend[some].astype(F32) + frecv[some].astype(F32)) * factor, lanes_u)

        @pl.when(c >= free)
        def _():
            put(mate * SPLIT + c - free, m, frecv[some].astype(F32) * factor, None)

    def energy(lanes):
        return jnp.sum(lanes[...].reshape(hidden_units, 128).T, axis=0, keepdims=True)

    def free_energy(to, slot):
        return pltpu.make_async_remote_copy(
            src_ref=esu, dst_ref=eru.at[slot], send_sem=us_sem.at[0], recv_sem=ur_sem.at[0],
            device_id={"fs": to}, device_id_type=MESH,
        )

    def split_energy(other, to, slot):
        return pltpu.make_async_remote_copy(
            src_ref=ess, dst_ref=ers.at[rep, slot], send_sem=ss_sem.at[other], recv_sem=sr_sem.at[other],
            device_id={"rep": jnp.where(other == 1, mate, rep), "fs": to}, device_id_type=MESH,
        )

    blocks = 4
    brows = tokens // blocks

    def activations(i):
        at_rows = pl.ds(pl.multiple_of(i * brows, brows), brows)
        gate = g[at_rows, :].astype(F32)
        up = u[at_rows, :].astype(F32)
        grad = dhid[at_rows, :]
        sig = jax.nn.sigmoid(gate)
        du[at_rows, :] = (grad * (gate * sig)).astype(BF16)
        dg[at_rows, :] = (grad * up * sig * (1.0 + gate * (1.0 - sig))).astype(BF16)

    def last(c, m, i):
        finish(c, m, i)

        @pl.when((i >= FROM) & (i < FROM + halves))
        def _():
            gather(1, i - FROM, ends=False)

        @pl.when((i >= FROM + halves) & (i < FROM + halves + n - 2))
        def _():
            loop(0, halves, functools.partial(gather, 2 + i - FROM - halves))

    steps(0, end - 1, last)
    steps(end - 1, end, finish)
    ess[...] = energy(lanes_s)
    for t in range(1, n):
        split_energy(0, lax.rem(k + t, n), k).start()
    for t in range(n):
        split_energy(1, lax.rem(k + t, n), k).start()

    def outputs():
        @pl.when((k == 0) | (k == n - 1))
        def _():
            loop(0, halves, functools.partial(gather, 1, ends=True))

        loop(0, blocks, activations)

    @pl.when(rep == FIRST)
    def _():
        outputs()

    steps(0, free // GROUP, deliver)
    esu[...] = energy(lanes_u)
    for t in range(1, n):
        free_energy(lax.rem(k + t, n), k).start()

    @pl.when(rep != FIRST)
    def _():
        outputs()

    steps(free // GROUP, end, deliver)

    for d in range(2):

        for p in range(n - 1):
            for r in range(2):

                @pl.when((at[d] == p) & (rep == r))
                def _():
                    sent = spread((p + 1) * count - r * d)
                    along(d, 0, 0, sent, sent).wait_send()
                    sent = zsend.at[d, pl.ds(0, n - 1 - p)]
                    along(d, 0, 0, sent, sent, 1).wait_send()

    across(fsend, frecv, fs_sem.at[0], fr_sem.at[0]).wait_send()
    across(ysend, yrecv, ys_sem.at[0], yr_sem.at[0]).wait_send()

    for r in range(2):

        @pl.when(((rep == 0) & (k < n - 1)) == (r == 1))
        def _():
            crossed = spread((n - 1) * SPLIT + r)
            across(crossed, crossed, as_sem.at[0], ar_sem.at[0]).wait_send()

    def settle(some, send, recv):
        copy = across(some, some, send, recv)
        copy.wait_send()
        copy.wait_recv()

    settle(eru.at[pl.ds(0, n - 1)], us_sem.at[0], ur_sem.at[0])
    settle(ers.at[0, pl.ds(0, n - 1)], ss_sem.at[0], sr_sem.at[0])
    settle(ers.at[1], ss_sem.at[1], sr_sem.at[1])
    total = jnp.zeros((1, hidden_units), F32)
    for j in range(n):
        total += jnp.where(j == k, esu[...], eru[j])
        for r in range(2):
            total += jnp.where((j == k) & (r == rep), ess[...], ers[r, j])
    en_ref[...] = total * (1.0 / width)


def write_out(dg, du, gd, en, dg_hbm, du_hbm, gd_hbm, en_hbm, flat, sem):
    def copy_of(i, src, dst):
        return pltpu.make_async_copy(src, dst, sem.at[i])

    copies = [copy_of(0, dg, dg_hbm), copy_of(1, du, du_hbm), copy_of(2, gd, gd_hbm)]
    for copy in copies:
        copy.start()
    flat[...] = en[0, :]
    copies.append(copy_of(3, flat, en_hbm))
    copies[3].start()
    for copy in copies:
        copy.wait()


def fused(n, gate_pre, up_pre, out_grad, w_down):
    tokens, units = gate_pre.shape
    width = out_grad.shape[1]
    cols = w_down.shape[1]
    rows = units // PIECES
    count = PIECES - SPLIT
    factor = float(tokens * lax.axis_size("rep") * n) ** (-0.5)
    any_spec = pl.BlockSpec(memory_space=pl.ANY)
    vmem_spec = pl.BlockSpec(memory_space=pltpu.VMEM)
    dma = pltpu.SemaphoreType.DMA
    d_gate, d_up, grad, energy = pl.pallas_call(
        functools.partial(kernel, n, factor, width),
        out_shape=(
            pltpu.VMEM((tokens, units), BF16),
            pltpu.VMEM((tokens, units), BF16),
            pltpu.VMEM((PIECES, rows, cols), F32),
            pltpu.VMEM((1, units), F32),
        ),
        in_specs=[any_spec] * 4,
        out_specs=(vmem_spec,) * 4,
        scratch_shapes=[
            pltpu.VMEM((tokens, units), BF16),
            pltpu.VMEM((tokens, units), BF16),
            pltpu.VMEM((n, tokens, cols), BF16),
            pltpu.VMEM((n, PIECES, rows, cols), BF16),
            pltpu.VMEM((units, tokens), BF16),
            pltpu.VMEM((n, PIECES, rows, cols), F32),
            pltpu.VMEM((tokens, units), F32),
            pltpu.VMEM((2, n - 1, count, rows, cols), BF16),
            pltpu.VMEM((2, n - 1, count, rows, cols), BF16),
            pltpu.VMEM((n, SPLIT, rows, cols), BF16),
            pltpu.VMEM((n, SPLIT, rows, cols), BF16),
            pltpu.VMEM((count, rows, cols), BF16),
            pltpu.VMEM((count, rows, cols), BF16),
            pltpu.VMEM((PIECES, rows, 128), F32),
            pltpu.VMEM((PIECES, rows, 128), F32),
            pltpu.VMEM((1, units), F32),
            pltpu.VMEM((n, 1, units), F32),
            pltpu.VMEM((1, units), F32),
            pltpu.VMEM((2, n, 1, units), F32),
            dma((4 + 2 * LOADS,)),
            dma((n,)),
            dma((2, 2)),
            dma((2, 2 * -(-count // GROUP) + 1)),
            dma((2,)),
            dma((1,)),
            dma((n,)),
            dma((1,)),
            dma((n,)),
            dma((1,)),
            dma((-(-count // GROUP),)),
            dma((1,)),
            dma((1,)),
            dma((2,)),
            dma((2,)),
        ],
        compiler_params=pltpu.CompilerParams(
            collective_id=0, has_side_effects=True, vmem_limit_bytes=VMEM_LIMIT
        ),
    )(gate_pre, up_pre, out_grad, w_down.reshape(PIECES, rows, cols))
    return pl.pallas_call(
        write_out,
        out_shape=(
            jax.ShapeDtypeStruct((tokens, units), BF16),
            jax.ShapeDtypeStruct((tokens, units), BF16),
            jax.ShapeDtypeStruct((units, cols), F32),
            jax.ShapeDtypeStruct((units,), F32),
        ),
        in_specs=[vmem_spec] * 4,
        out_specs=(any_spec,) * 4,
        scratch_shapes=[pltpu.VMEM((units,), F32), dma((4,))],
        compiler_params=pltpu.CompilerParams(vmem_limit_bytes=4 * 1024 * 1024),
    )(d_gate, d_up, grad.reshape(units, cols), energy)


def solution(mesh):
    reps, n = mesh.shape["rep"], mesh.shape["fs"]

    def local(gate_pre, up_pre, out_grad, w_down):
        units, cols = w_down.shape
        fits = reps == 2 and 2 <= n <= 4 and cols % 128 == 0 and units % (PIECES * 16) == 0 and units % 128 == 0
        if fits and gate_pre.shape[0] % 1024 == 0:
            return fused(n, gate_pre, up_pre, out_grad, w_down)
        return plain(gate_pre, up_pre, out_grad, w_down)

    placed = (P(("rep", "fs"), "tp"), P(("rep", "fs"), "tp"), P(("rep", "fs"), None), P("tp", "fs"))
    return jax.shard_map(
        local,
        mesh=mesh,
        in_specs=placed,
        out_specs=(P(("rep", "fs"), "tp"), P(("rep", "fs"), "tp"), P("tp", "fs"), P("tp")),
        check_vma=False,
    )
```

```python
import functools

import jax
import jax.numpy as jnp
from jax import lax
from jax.experimental import pallas as pl
from jax.experimental.pallas import tpu as pltpu
from jax.sharding import PartitionSpec as P

MESH = pl.DeviceIdType.MESH
F32 = jnp.float32
BF16 = jnp.bfloat16
PIECES = 16
SPLIT = 5
GROUP = 2
FIRST = 2
FROM = 1
LOADS = 4
BEFORE = 0
VMEM_LIMIT = 52 * 1024 * 1024


def plain(gate_pre, up_pre, out_grad, w_down):
    gate_f = gate_pre.astype(F32)
    up_f = up_pre.astype(F32)
    sig = jax.nn.sigmoid(gate_f)
    act = gate_f * sig
    hidden = (act * up_f).astype(BF16)
    tokens_all = out_grad.shape[0] * lax.axis_size("rep") * lax.axis_size("fs")
    factor = float(tokens_all) ** (-0.5)
    weight_whole = lax.all_gather(w_down, "fs", axis=1, tiled=True)
    dhid = lax.dot_general(out_grad, weight_whole, (((1,), (1,)), ((), ())), preferred_element_type=F32)
    d_up = (dhid * act).astype(BF16)
    d_gate = (dhid * up_f * sig * (1.0 + gate_f * (1.0 - sig))).astype(BF16)
    shard = lax.psum_scatter(
        lax.dot_general(out_grad, hidden, (((0,), (0,)), ((), ())), preferred_element_type=F32),
        "fs",
        scatter_dimension=0,
        tiled=True,
    )
    shard = lax.psum(shard, "rep")
    grad_down = shard.T * factor
    energy = lax.psum(jnp.sum(grad_down * grad_down, axis=1), "fs") / out_grad.shape[1]
    return (d_gate, d_up, grad_down, energy)


def kernel(
    n, factor, width,
    g_hbm, u_hbm, og_hbm, w_hbm,
    dg, du, gd, en_ref,
    g, u, og, w, hid, part, dhid, zsend, zrecv, ysend, yrecv, fsend, frecv,
    lanes_u, lanes_s, esu, eru, ess, ers,
    in_sem, og_sem, zs_sem, zr_sem, zx_sem, as_sem, ar_sem, ys_sem, yr_sem, fs_sem, fr_sem,
    us_sem, ur_sem, ss_sem, sr_sem,
):
    rep = lax.axis_index("rep")
    k = lax.axis_index("fs")
    mate = 1 - rep
    cols = w.shape[3]
    rows = w.shape[2]
    hidden_units = g.shape[1]
    tokens = g.shape[0]
    count = PIECES - SPLIT
    free = PIECES - 2 * SPLIT
    pairs = count // GROUP
    chunk = tokens // LOADS

    def piece(c):
        return c + jnp.where(c < free, 2 * SPLIT, rep * SPLIT - free)

    def loop(lo, hi, body):
        lax.fori_loop(lo, hi, lambda i, x: (body(i), x)[1], 0)

    def steps(lo, hi, body):
        loop(lo, min(hi, pairs), lambda i: body(GROUP * i, GROUP, i))
        if hi > pairs:
            body(k * 0 + GROUP * pairs, count % GROUP, k * 0 + pairs)

    end = -(-count // GROUP)
    late = free // GROUP - 1
    low = jnp.minimum(k, n - 1 - k)

    def chosen(i):
        far = jnp.where(i < n - 1 - low, n - 1 - i, jnp.where(i < n - 1, i - (n - 1 - low), low))
        return jnp.where(2 * k >= n, n - 1 - far, far)

    def rows_at(i):
        return pl.ds(pl.multiple_of(i * chunk, chunk), chunk)

    wide = -(-2 * SPLIT * rows // 128) * 128
    spans = ((0, wide), (wide, hidden_units - wide)) if wide < hidden_units else ((0, wide),)

    def in_gate(h, i):
        at = (rows_at(i) if h == 0 else pl.ds(0, tokens), pl.ds(*spans[h]))
        return pltpu.make_async_copy(g_hbm.at[at], g.at[at], in_sem.at[3 + i if h == 0 else 2])

    def in_up(h, i):
        at = (rows_at(i) if h == 0 else pl.ds(0, tokens), pl.ds(*spans[h]))
        return pltpu.make_async_copy(u_hbm.at[at], u.at[at], in_sem.at[3 + i if h == 0 else 2])

    def in_og(j):
        part_of = pl.ds(pl.multiple_of(j * cols, cols), cols)
        return pltpu.make_async_copy(og_hbm.at[:, part_of], og.at[j], og_sem.at[j])

    at = (k, n - 1 - k)
    sign = (1, -1)

    barrier = pltpu.get_barrier_semaphore()
    for d in range(2):

        @pl.when(at[d] < n - 1)
        def _():
            pl.semaphore_signal(barrier, inc=1, device_id={"fs": k + sign[d]}, device_id_type=MESH)

    pl.semaphore_signal(barrier, inc=1, device_id={"rep": mate}, device_id_type=MESH)
    in_w = [
        pltpu.make_async_copy(w_hbm.at[some], w.at[k, some], in_sem.at[i])
        for i, some in enumerate((pl.ds(2 * SPLIT, free), pl.ds(0, 2 * SPLIT)))
    ]
    for copy in in_w:
        copy.start()

    def load(h, i):
        in_gate(h, i).start()
        in_up(h, i).start()

    loop(0, LOADS, functools.partial(load, 0))
    in_og(chosen(0)).start()
    for h in range(1, len(spans)):
        load(h, 0)
    loop(1, n, lambda i: in_og(chosen(i)).start())
    def along(d, s, i, src, dst, kind=0):
        return pltpu.make_async_remote_copy(
            src_ref=src, dst_ref=dst, send_sem=zs_sem.at[d, kind], recv_sem=zr_sem.at[d, lax.rem(s * end + i, 2 * end + 1)],
            device_id={"fs": k + sign[d]}, device_id_type=MESH,
        )

    def block_of(j, p, m, i):
        brief = (i == 0) & (rep == 1) & (j == n - 1)

        def each_size(act):
            @pl.when(brief)
            def _():
                act(w.at[j, pl.ds(p, m - 1)])

            @pl.when(jnp.logical_not(brief))
            def _():
                act(w.at[j, pl.ds(p, m)])

        return each_size

    def spread(pieces):
        blocks = next(b for b in range(1, n + 1) if pieces % b == 0 and pieces // b <= PIECES)
        return w.at[pl.ds(0, blocks), pl.ds(0, pieces // blocks)]

    def send_block(d, s, i, j, p, m):
        if m > 1:
            block_of(j, p, m, i)(lambda block: along(d, s, i, block, block).start())
        else:
            block = w.at[j, pl.ds(p, m)]
            along(d, s, i, block, block).start()

    def take_block(d, s, i, j, p, m):
        if m > 1:
            block_of(j, p, m, i)(lambda block: along(d, s, i, block, block).wait_recv())
        else:
            block = w.at[j, pl.ds(p, m)]
            along(d, s, i, block, block).wait_recv()

    def deferred(d):
        block = w.at[k, pl.ds(2 * SPLIT + late * GROUP, GROUP)]
        return pltpu.make_async_remote_copy(
            src_ref=block, dst_ref=block, send_sem=zs_sem.at[d, 0], recv_sem=zx_sem.at[d],
            device_id={"fs": k + sign[d]}, device_id_type=MESH,
        )

    def across(src, dst, send, recv):
        return pltpu.make_async_remote_copy(
            src_ref=src, dst_ref=dst, send_sem=send, recv_sem=recv,
            device_id={"rep": mate}, device_id_type=MESH,
        )

    def early(j):
        return across(ysend.at[j], yrecv.at[j], ys_sem.at[0], yr_sem.at[j])

    def final(c, m, i):
        return across(fsend.at[pl.ds(c, m)], frecv.at[pl.ds(c, m)], fs_sem.at[0], fr_sem.at[(i >= free // GROUP).astype(jnp.int32)])

    def crossing(j, owner, start, m):
        block = w.at[j, pl.ds(owner * SPLIT + start, m)]
        return across(block, block, as_sem.at[0], ar_sem.at[j])

    def loaded(h, i):
        both = (pl.ds(0, 2 * chunk), pl.ds(*spans[0])) if h == 0 else (pl.ds(0, tokens), pl.ds(0, 2 * spans[h][1]))
        sem = in_sem.at[3 + i if h == 0 else 2]
        pltpu.make_async_copy(g_hbm.at[both], g.at[both], sem).wait()

    def make_hidden(h, i):
        if h == 0:
            loaded(h, i)
        start, width = spans[h]
        at = (rows_at(i), pl.ds(start, width))
        gate = g[at].astype(F32)
        act = gate * jax.nn.sigmoid(gate)
        hid[pl.ds(start, width), rows_at(i)] = (act * u[at].astype(F32)).astype(BF16).T

    loop(0, BEFORE, functools.partial(make_hidden, 0))
    pl.semaphore_wait(barrier, 1 + (k > 0).astype(jnp.int32) + (k < n - 1).astype(jnp.int32))
    in_w[0].wait()

    def first(c, m, i):
        for d in range(2):

            @pl.when((at[d] < n - 2) | ((at[d] == n - 2) & (i != late)))
            def _():
                send_block(d, 0, i, k, piece(c), m)

    steps(0, free // GROUP, first)
    in_w[1].wait()
    steps(free // GROUP, end, first)
    loop(BEFORE, LOADS, functools.partial(make_hidden, 0))

    def product(j, start, pieces):
        some = hid[pl.ds(pl.multiple_of(start * rows, rows), pieces * rows), :]
        return jnp.dot(some, og[j], preferred_element_type=F32).reshape(pieces, rows, cols)

    def make_early(i):
        j = chosen(i)
        in_og(j).wait()
        ysend[j] = product(j, mate * SPLIT, SPLIT).astype(BF16)
        early(j).start()

    def make_part(j):
        part[j, pl.ds(2 * SPLIT, free)] = product(j, 2 * SPLIT, free)
        part[j, pl.ds(rep * SPLIT, SPLIT)] = product(j, rep * SPLIT, SPLIT)

    loop(0, n, make_early)
    for h in range(1, len(spans)):
        loaded(h, 0)
        loop(0, LOADS, functools.partial(make_hidden, h))
    loop(0, n, make_part)
    lanes_u[...] = jnp.zeros_like(lanes_u)
    lanes_s[...] = jnp.zeros_like(lanes_s)

    def multiply(j, at_rows):
        return lax.dot_general(
            og[j, at_rows, :], w[j].reshape(hidden_units, cols), (((1,), (1,)), ((), ())),
            preferred_element_type=F32,
        )

    def own(i):
        at_rows = pl.ds(pl.multiple_of(i * 256, 256), 256)
        dhid[at_rows, :] = multiply(k, at_rows)

    loop(0, tokens // 256, own)

    def pass_on(s, c, m, i):
        p = piece(c)
        for d in range(2):
            place = at[d]
            some = pl.ds(c, m)

            came = place > 0
            if s == 1:
                came &= (place < n - 1) | (i != late)

            @pl.when(came & (s > place))
            def _():
                along(d, s - 1, i, zsend.at[d, 0, some], zrecv.at[d, 0, some]).wait_recv()

            @pl.when(s <= place)
            def _():
                j = k - sign[d] * s

                @pl.when(came)
                def _():
                    take_block(d, s - 1, i, j, p, m)

                @pl.when(place < n - 1)
                def _():
                    send_block(d, s, i, j, p, m)

                @pl.when(c >= free)
                def _():
                    crossing(j, rep, c - free, m).start()

                @pl.when((i == 0) & (rep == 0) & (j == n - 1))
                def _():
                    extra = w.at[j, pl.ds(2 * SPLIT + GROUP - 1, 1)]
                    across(extra, extra, as_sem.at[0], ar_sem.at[j]).start()

            @pl.when(s > place)
            def _():
                j = k + sign[d] * (n - s)

                @pl.when(c == free)
                def _():
                    early(j).wait_recv()

                @pl.when(c >= free)
                def _():
                    part[j, pl.ds(p, m)] += yrecv[j, pl.ds(jnp.maximum(c - free, 0), m)].astype(F32)

                if s > 1:

                    @pl.when(place > 0)
                    def _():
                        part[j, pl.ds(p, m)] += zrecv[d, s - 2, some].astype(F32)

                zsend[d, s - 1, some] = part[j, pl.ds(p, m)].astype(BF16)
                along(d, s, i, zsend.at[d, s - 1, some], zrecv.at[d, s - 1, some], 1).start()

    def gathered(j):
        for r in range(2):

            @pl.when(((rep == 1) & (j == n - 1)) == (r == 1))
            def _():
                some = w.at[j, pl.ds(0, SPLIT + r)]
                across(some, some, as_sem.at[0], ar_sem.at[j]).wait_recv()

    halves = 2
    half = tokens // halves

    def gather(far, part_of, ends=None):
        at_rows = pl.ds(pl.multiple_of(part_of * half, half), half)
        for d in range(2):
            here = at[d] >= far
            if ends is not None:
                here &= (at[d] == n - 1) == ends

            @pl.when(here)
            def _():
                j = k - sign[d] * far

                @pl.when(part_of == 0)
                def _():
                    gathered(j)
                    if ends:
                        deferred(d).wait_recv()

                dhid[at_rows, :] += multiply(j, at_rows)

    for s in range(1, n - 1):
        steps(0, end, functools.partial(pass_on, s))
    steps(0, end, functools.partial(pass_on, n - 1))
    for d in range(2):

        @pl.when(at[d] == n - 2)
        def _():
            deferred(d).start()

    def put(p, m, value, lanes):
        gd[pl.ds(p, m)] = value
        if lanes is not None:
            sq = value * value
            total = sq[:, :, :128]
            for b in range(1, cols // 128):
                total += sq[:, :, b * 128 : (b + 1) * 128]
            lanes[pl.ds(p, m)] = total

    def finish(c, m, i):
        p = piece(c)
        some = pl.ds(c, m)

        @pl.when(c == free)
        def _():
            early(k).wait_recv()

        @pl.when(c >= free)
        def _():
            part[k, pl.ds(p, m)] += yrecv[k, pl.ds(jnp.maximum(c - free, 0), m)].astype(F32)

        for d in range(2):

            @pl.when(at[d] > 0)
            def _():
                along(d, n - 1, i, zsend.at[d, n - 2, some], zrecv.at[d, n - 2, some]).wait_recv()
                part[k, pl.ds(p, m)] += zrecv[d, n - 2, some].astype(F32)

        fsend[some] = part[k, pl.ds(p, m)].astype(BF16)
        final(c, m, i).start()

        @pl.when(c >= free)
        def _():
            put(p, m, fsend[some].astype(F32) * factor, lanes_s)

    def deliver(c, m, i):
        some = pl.ds(c, m)

        @pl.when(c < free)
        def _():
            put(piece(c), m, (fsend[some].astype(F32) + frecv[some].astype(F32)) * factor, lanes_u)

        @pl.when(c >= free)
        def _():
            put(mate * SPLIT + c - free, m, frecv[some].astype(F32) * factor, None)

    def energy(lanes):
        return jnp.sum(lanes[...].reshape(hidden_units, 128).T, axis=0, keepdims=True)

    def free_energy(to, slot):
        return pltpu.make_async_remote_copy(
            src_ref=esu, dst_ref=eru.at[slot], send_sem=us_sem.at[0], recv_sem=ur_sem.at[0],
            device_id={"fs": to}, device_id_type=MESH,
        )

    def split_energy(other, to, slot):
        return pltpu.make_async_remote_copy(
            src_ref=ess, dst_ref=ers.at[rep, slot], send_sem=ss_sem.at[other], recv_sem=sr_sem.at[other],
            device_id={"rep": jnp.where(other == 1, mate, rep), "fs": to}, device_id_type=MESH,
        )

    blocks = 4
    brows = tokens // blocks

    def activations(i):
        at_rows = pl.ds(pl.multiple_of(i * brows, brows), brows)
        gate = g[at_rows, :].astype(F32)
        up = u[at_rows, :].astype(F32)
        grad = dhid[at_rows, :]
        sig = jax.nn.sigmoid(gate)
        du[at_rows, :] = (grad * (gate * sig)).astype(BF16)
        dg[at_rows, :] = (grad * up * sig * (1.0 + gate * (1.0 - sig))).astype(BF16)

    def last(c, m, i):
        finish(c, m, i)

        @pl.when((i >= FROM) & (i < FROM + halves))
        def _():
            gather(1, i - FROM, ends=False)

        @pl.when((i >= FROM + halves) & (i < FROM + halves + n - 2))
        def _():
            loop(0, halves, functools.partial(gather, 2 + i - FROM - halves))

    steps(0, end - 1, last)
    steps(end - 1, end, finish)
    ess[...] = energy(lanes_s)
    for t in range(1, n):
        split_energy(0, lax.rem(k + t, n), k).start()
    for t in range(n):
        split_energy(1, lax.rem(k + t, n), k).start()

    def outputs():
        @pl.when((k == 0) | (k == n - 1))
        def _():
            loop(0, halves, functools.partial(gather, 1, ends=True))

        loop(0, blocks, activations)

    @pl.when(rep == FIRST)
    def _():
        outputs()

    def arrived(start, pieces, slot):
        some = pl.ds(start, pieces)
        across(fsend.at[some], frecv.at[some], fs_sem.at[0], fr_sem.at[slot]).wait_recv()

    arrived(0, free, 0)
    steps(0, free // GROUP, deliver)
    esu[...] = energy(lanes_u)
    for t in range(1, n):
        free_energy(lax.rem(k + t, n), k).start()

    @pl.when(rep != FIRST)
    def _():
        outputs()

    arrived(free, SPLIT, 1)
    steps(free // GROUP, end, deliver)

    for d in range(2):

        for p in range(n - 1):
            for r in range(2):

                @pl.when((at[d] == p) & (rep == r))
                def _():
                    sent = spread((p + 1) * count - r * d)
                    along(d, 0, 0, sent, sent).wait_send()
                    sent = zsend.at[d, pl.ds(0, n - 1 - p)]
                    along(d, 0, 0, sent, sent, 1).wait_send()

    across(fsend, frecv, fs_sem.at[0], fr_sem.at[0]).wait_send()
    across(ysend, yrecv, ys_sem.at[0], yr_sem.at[0]).wait_send()

    for r in range(2):

        @pl.when(((rep == 0) & (k < n - 1)) == (r == 1))
        def _():
            crossed = spread((n - 1) * SPLIT + r)
            across(crossed, crossed, as_sem.at[0], ar_sem.at[0]).wait_send()

    def settle(some, send, recv):
        copy = across(some, some, send, recv)
        copy.wait_send()
        copy.wait_recv()

    settle(eru.at[pl.ds(0, n - 1)], us_sem.at[0], ur_sem.at[0])
    settle(ers.at[0, pl.ds(0, n - 1)], ss_sem.at[0], sr_sem.at[0])
    settle(ers.at[1], ss_sem.at[1], sr_sem.at[1])
    total = jnp.zeros((1, hidden_units), F32)
    for j in range(n):
        total += jnp.where(j == k, esu[...], eru[j])
        for r in range(2):
            total += jnp.where((j == k) & (r == rep), ess[...], ers[r, j])
    en_ref[...] = total * (1.0 / width)


def write_out(dg, du, gd, en, dg_hbm, du_hbm, gd_hbm, en_hbm, flat, sem):
    def copy_of(i, src, dst):
        return pltpu.make_async_copy(src, dst, sem.at[i])

    copies = [copy_of(0, dg, dg_hbm), copy_of(1, du, du_hbm), copy_of(2, gd, gd_hbm)]
    for copy in copies:
        copy.start()
    flat[...] = en[0, :]
    copies.append(copy_of(3, flat, en_hbm))
    copies[3].start()
    for copy in copies:
        copy.wait()


def fused(n, gate_pre, up_pre, out_grad, w_down):
    tokens, units = gate_pre.shape
    width = out_grad.shape[1]
    cols = w_down.shape[1]
    rows = units // PIECES
    count = PIECES - SPLIT
    factor = float(tokens * lax.axis_size("rep") * n) ** (-0.5)
    any_spec = pl.BlockSpec(memory_space=pl.ANY)
    vmem_spec = pl.BlockSpec(memory_space=pltpu.VMEM)
    dma = pltpu.SemaphoreType.DMA
    d_gate, d_up, grad, energy = pl.pallas_call(
        functools.partial(kernel, n, factor, width),
        out_shape=(
            pltpu.VMEM((tokens, units), BF16),
            pltpu.VMEM((tokens, units), BF16),
            pltpu.VMEM((PIECES, rows, cols), F32),
            pltpu.VMEM((1, units), F32),
        ),
        in_specs=[any_spec] * 4,
        out_specs=(vmem_spec,) * 4,
        scratch_shapes=[
            pltpu.VMEM((tokens, units), BF16),
            pltpu.VMEM((tokens, units), BF16),
            pltpu.VMEM((n, tokens, cols), BF16),
            pltpu.VMEM((n, PIECES, rows, cols), BF16),
            pltpu.VMEM((units, tokens), BF16),
            pltpu.VMEM((n, PIECES, rows, cols), F32),
            pltpu.VMEM((tokens, units), F32),
            pltpu.VMEM((2, n - 1, count, rows, cols), BF16),
            pltpu.VMEM((2, n - 1, count, rows, cols), BF16),
            pltpu.VMEM((n, SPLIT, rows, cols), BF16),
            pltpu.VMEM((n, SPLIT, rows, cols), BF16),
            pltpu.VMEM((count, rows, cols), BF16),
            pltpu.VMEM((count, rows, cols), BF16),
            pltpu.VMEM((PIECES, rows, 128), F32),
            pltpu.VMEM((PIECES, rows, 128), F32),
            pltpu.VMEM((1, units), F32),
            pltpu.VMEM((n, 1, units), F32),
            pltpu.VMEM((1, units), F32),
            pltpu.VMEM((2, n, 1, units), F32),
            dma((3 + LOADS,)),
            dma((n,)),
            dma((2, 2)),
            dma((2, 2 * -(-count // GROUP) + 1)),
            dma((2,)),
            dma((1,)),
            dma((n,)),
            dma((1,)),
            dma((n,)),
            dma((1,)),
            dma((2,)),
            dma((1,)),
            dma((1,)),
            dma((2,)),
            dma((2,)),
        ],
        compiler_params=pltpu.CompilerParams(
            collective_id=0, has_side_effects=True, vmem_limit_bytes=VMEM_LIMIT
        ),
    )(gate_pre, up_pre, out_grad, w_down.reshape(PIECES, rows, cols))
    return pl.pallas_call(
        write_out,
        out_shape=(
            jax.ShapeDtypeStruct((tokens, units), BF16),
            jax.ShapeDtypeStruct((tokens, units), BF16),
            jax.ShapeDtypeStruct((units, cols), F32),
            jax.ShapeDtypeStruct((units,), F32),
        ),
        in_specs=[vmem_spec] * 4,
        out_specs=(any_spec,) * 4,
        scratch_shapes=[pltpu.VMEM((units,), F32), dma((4,))],
        compiler_params=pltpu.CompilerParams(vmem_limit_bytes=4 * 1024 * 1024),
    )(d_gate, d_up, grad.reshape(units, cols), energy)


def solution(mesh):
    reps, n = mesh.shape["rep"], mesh.shape["fs"]

    def local(gate_pre, up_pre, out_grad, w_down):
        units, cols = w_down.shape
        fits = reps == 2 and 2 <= n <= 4 and cols % 128 == 0 and units % (PIECES * 16) == 0 and units % 128 == 0
        if fits and gate_pre.shape[0] % 1024 == 0:
            return fused(n, gate_pre, up_pre, out_grad, w_down)
        return plain(gate_pre, up_pre, out_grad, w_down)

    placed = (P(("rep", "fs"), "tp"), P(("rep", "fs"), "tp"), P(("rep", "fs"), None), P("tp", "fs"))
    return jax.shard_map(
        local,
        mesh=mesh,
        in_specs=placed,
        out_specs=(P(("rep", "fs"), "tp"), P(("rep", "fs"), "tp"), P("tp", "fs"), P("tp")),
        check_vma=False,
    )
```

```python
import functools

import jax
import jax.numpy as jnp
from jax import lax
from jax.experimental import pallas as pl
from jax.experimental.pallas import tpu as pltpu
from jax.sharding import PartitionSpec as P

MESH = pl.DeviceIdType.MESH
F32 = jnp.float32
BF16 = jnp.bfloat16
PIECES = 16
SPLIT = 5
GROUP = 2
FIRST = 2
FROM = 1
LOADS = 4
BEFORE = 0
VMEM_LIMIT = 52 * 1024 * 1024


def plain(gate_pre, up_pre, out_grad, w_down):
    gate_f = gate_pre.astype(F32)
    up_f = up_pre.astype(F32)
    sig = jax.nn.sigmoid(gate_f)
    act = gate_f * sig
    hidden = (act * up_f).astype(BF16)
    tokens_all = out_grad.shape[0] * lax.axis_size("rep") * lax.axis_size("fs")
    factor = float(tokens_all) ** (-0.5)
    weight_whole = lax.all_gather(w_down, "fs", axis=1, tiled=True)
    dhid = lax.dot_general(out_grad, weight_whole, (((1,), (1,)), ((), ())), preferred_element_type=F32)
    d_up = (dhid * act).astype(BF16)
    d_gate = (dhid * up_f * sig * (1.0 + gate_f * (1.0 - sig))).astype(BF16)
    shard = lax.psum_scatter(
        lax.dot_general(out_grad, hidden, (((0,), (0,)), ((), ())), preferred_element_type=F32),
        "fs",
        scatter_dimension=0,
        tiled=True,
    )
    shard = lax.psum(shard, "rep")
    grad_down = shard.T * factor
    energy = lax.psum(jnp.sum(grad_down * grad_down, axis=1), "fs") / out_grad.shape[1]
    return (d_gate, d_up, grad_down, energy)


def kernel(
    n, factor, width,
    g_hbm, u_hbm, og_hbm, w_hbm,
    dg, du, gd, en_ref,
    g, u, og, w, hid, part, dhid, zsend, zrecv, ysend, yrecv, fsend, frecv,
    lanes_u, lanes_s, esu, eru, ess, ers,
    in_sem, og_sem, zs_sem, zr_sem, zx_sem, as_sem, ar_sem, ys_sem, yr_sem, fs_sem, fr_sem,
    us_sem, ur_sem, ss_sem, sr_sem,
):
    rep = lax.axis_index("rep")
    k = lax.axis_index("fs")
    mate = 1 - rep
    cols = w.shape[3]
    rows = w.shape[2]
    hidden_units = g.shape[1]
    tokens = g.shape[0]
    count = PIECES - SPLIT
    free = PIECES - 2 * SPLIT
    pairs = count // GROUP
    chunk = tokens // LOADS

    def piece(c):
        return c + jnp.where(c < free, 2 * SPLIT, rep * SPLIT - free)

    def loop(lo, hi, body):
        lax.fori_loop(lo, hi, lambda i, x: (body(i), x)[1], 0)

    def steps(lo, hi, body):
        loop(lo, min(hi, pairs), lambda i: body(GROUP * i, GROUP, i))
        if hi > pairs:
            body(k * 0 + GROUP * pairs, count % GROUP, k * 0 + pairs)

    end = -(-count // GROUP)
    late = free // GROUP - 1
    low = jnp.minimum(k, n - 1 - k)

    def chosen(i):
        far = jnp.where(i < n - 1 - low, n - 1 - i, jnp.where(i < n - 1, i - (n - 1 - low), low))
        return jnp.where(2 * k >= n, n - 1 - far, far)

    def rows_at(i):
        return pl.ds(pl.multiple_of(i * chunk, chunk), chunk)

    wide = -(-2 * SPLIT * rows // 128) * 128
    spans = ((0, wide), (wide, hidden_units - wide)) if wide < hidden_units else ((0, wide),)

    def in_gate(h, i):
        at = (rows_at(i) if h == 0 else pl.ds(0, tokens), pl.ds(*spans[h]))
        return pltpu.make_async_copy(g_hbm.at[at], g.at[at], in_sem.at[3 + i if h == 0 else 2])

    def in_up(h, i):
        at = (rows_at(i) if h == 0 else pl.ds(0, tokens), pl.ds(*spans[h]))
        return pltpu.make_async_copy(u_hbm.at[at], u.at[at], in_sem.at[3 + i if h == 0 else 2])

    def in_og(j):
        part_of = pl.ds(pl.multiple_of(j * cols, cols), cols)
        return pltpu.make_async_copy(og_hbm.at[:, part_of], og.at[j], og_sem.at[j])

    at = (k, n - 1 - k)
    sign = (1, -1)

    barrier = pltpu.get_barrier_semaphore()
    for d in range(2):

        @pl.when(at[d] < n - 1)
        def _():
            pl.semaphore_signal(barrier, inc=1, device_id={"fs": k + sign[d]}, device_id_type=MESH)

    pl.semaphore_signal(barrier, inc=1, device_id={"rep": mate}, device_id_type=MESH)
    in_w = [
        pltpu.make_async_copy(w_hbm.at[some], w.at[k, some], in_sem.at[i])
        for i, some in enumerate((pl.ds(2 * SPLIT, free), pl.ds(0, 2 * SPLIT)))
    ]
    for copy in in_w:
        copy.start()

    def load(h, i):
        in_gate(h, i).start()
        in_up(h, i).start()

    loop(0, LOADS, functools.partial(load, 0))
    in_og(chosen(0)).start()
    for h in range(1, len(spans)):
        load(h, 0)
    loop(1, n, lambda i: in_og(chosen(i)).start())
    def along(d, s, i, src, dst, kind=0):
        return pltpu.make_async_remote_copy(
            src_ref=src, dst_ref=dst, send_sem=zs_sem.at[d, kind], recv_sem=zr_sem.at[d, lax.rem(s * end + i, 2 * end + 1)],
            device_id={"fs": k + sign[d]}, device_id_type=MESH,
        )

    def block_of(j, p, m, i):
        brief = (i == 0) & (rep == 1) & (j == n - 1)

        def each_size(act):
            @pl.when(brief)
            def _():
                act(w.at[j, pl.ds(p, m - 1)])

            @pl.when(jnp.logical_not(brief))
            def _():
                act(w.at[j, pl.ds(p, m)])

        return each_size

    def spread(pieces):
        blocks = next(b for b in range(1, n + 1) if pieces % b == 0 and pieces // b <= PIECES)
        return w.at[pl.ds(0, blocks), pl.ds(0, pieces // blocks)]

    def send_block(d, s, i, j, p, m):
        if m > 1:
            block_of(j, p, m, i)(lambda block: along(d, s, i, block, block).start())
        else:
            block = w.at[j, pl.ds(p, m)]
            along(d, s, i, block, block).start()

    def take_block(d, s, i, j, p, m):
        if m > 1:
            block_of(j, p, m, i)(lambda block: along(d, s, i, block, block).wait_recv())
        else:
            block = w.at[j, pl.ds(p, m)]
            along(d, s, i, block, block).wait_recv()

    def deferred(d):
        block = w.at[k, pl.ds(2 * SPLIT + late * GROUP, GROUP)]
        return pltpu.make_async_remote_copy(
            src_ref=block, dst_ref=block, send_sem=zs_sem.at[d, 0], recv_sem=zx_sem.at[d],
            device_id={"fs": k + sign[d]}, device_id_type=MESH,
        )

    def across(src, dst, send, recv):
        return pltpu.make_async_remote_copy(
            src_ref=src, dst_ref=dst, send_sem=send, recv_sem=recv,
            device_id={"rep": mate}, device_id_type=MESH,
        )

    def early(j):
        return across(ysend.at[j], yrecv.at[j], ys_sem.at[0], yr_sem.at[j])

    def final(c, m, i):
        return across(fsend.at[pl.ds(c, m)], frecv.at[pl.ds(c, m)], fs_sem.at[0], fr_sem.at[(i >= free // GROUP).astype(jnp.int32)])

    def crossing(j, owner, start, m):
        block = w.at[j, pl.ds(owner * SPLIT + start, m)]
        return across(block, block, as_sem.at[0], ar_sem.at[j])

    def loaded(h, i):
        both = (pl.ds(0, 2 * chunk), pl.ds(*spans[0])) if h == 0 else (pl.ds(0, tokens), pl.ds(0, 2 * spans[h][1]))
        sem = in_sem.at[3 + i if h == 0 else 2]
        pltpu.make_async_copy(g_hbm.at[both], g.at[both], sem).wait()

    def make_hidden(h, i):
        if h == 0:
            loaded(h, i)
        start, width = spans[h]
        at = (rows_at(i), pl.ds(start, width))
        gate = g[at].astype(F32)
        act = gate * jax.nn.sigmoid(gate)
        hid[pl.ds(start, width), rows_at(i)] = (act * u[at].astype(F32)).astype(BF16).T

    loop(0, BEFORE, functools.partial(make_hidden, 0))
    pl.semaphore_wait(barrier, 1 + (k > 0).astype(jnp.int32) + (k < n - 1).astype(jnp.int32))
    in_w[0].wait()

    def first(c, m, i):
        for d in range(2):

            @pl.when((at[d] < n - 2) | ((at[d] == n - 2) & (i != late)))
            def _():
                send_block(d, 0, i, k, piece(c), m)

    steps(0, free // GROUP, first)
    in_w[1].wait()
    steps(free // GROUP, end, first)
    loop(BEFORE, LOADS, functools.partial(make_hidden, 0))

    def product(j, start, pieces):
        some = hid[pl.ds(pl.multiple_of(start * rows, rows), pieces * rows), :]
        return jnp.dot(some, og[j], preferred_element_type=F32).reshape(pieces, rows, cols)

    def make_early(i):
        j = chosen(i)
        in_og(j).wait()
        ysend[j] = product(j, mate * SPLIT, SPLIT).astype(BF16)
        early(j).start()

    def make_part(j):
        part[j, pl.ds(2 * SPLIT, free)] = product(j, 2 * SPLIT, free)
        part[j, pl.ds(rep * SPLIT, SPLIT)] = product(j, rep * SPLIT, SPLIT)

    loop(0, n, make_early)
    for h in range(1, len(spans)):
        loaded(h, 0)
        loop(0, LOADS, functools.partial(make_hidden, h))
    loop(0, n, make_part)
    lanes_u[...] = jnp.zeros_like(lanes_u)
    esu[...] = jnp.zeros_like(esu)
    lanes_s[...] = jnp.zeros_like(lanes_s)

    def multiply(j, at_rows):
        return lax.dot_general(
            og[j, at_rows, :], w[j].reshape(hidden_units, cols), (((1,), (1,)), ((), ())),
            preferred_element_type=F32,
        )

    def own(i):
        at_rows = pl.ds(pl.multiple_of(i * 256, 256), 256)
        dhid[at_rows, :] = multiply(k, at_rows)

    loop(0, tokens // 256, own)

    def pass_on(s, c, m, i):
        p = piece(c)
        for d in range(2):
            place = at[d]
            some = pl.ds(c, m)

            came = place > 0
            if s == 1:
                came &= (place < n - 1) | (i != late)

            @pl.when(came & (s > place))
            def _():
                along(d, s - 1, i, zsend.at[d, 0, some], zrecv.at[d, 0, some]).wait_recv()

            @pl.when(s <= place)
            def _():
                j = k - sign[d] * s

                @pl.when(came)
                def _():
                    take_block(d, s - 1, i, j, p, m)

                @pl.when(place < n - 1)
                def _():
                    send_block(d, s, i, j, p, m)

                @pl.when(c >= free)
                def _():
                    crossing(j, rep, c - free, m).start()

                @pl.when((i == 0) & (rep == 0) & (j == n - 1))
                def _():
                    extra = w.at[j, pl.ds(2 * SPLIT + GROUP - 1, 1)]
                    across(extra, extra, as_sem.at[0], ar_sem.at[j]).start()

            @pl.when(s > place)
            def _():
                j = k + sign[d] * (n - s)

                @pl.when(c == free)
                def _():
                    early(j).wait_recv()

                @pl.when(c >= free)
                def _():
                    part[j, pl.ds(p, m)] += yrecv[j, pl.ds(jnp.maximum(c - free, 0), m)].astype(F32)

                if s > 1:

                    @pl.when(place > 0)
                    def _():
                        part[j, pl.ds(p, m)] += zrecv[d, s - 2, some].astype(F32)

                zsend[d, s - 1, some] = part[j, pl.ds(p, m)].astype(BF16)
                along(d, s, i, zsend.at[d, s - 1, some], zrecv.at[d, s - 1, some], 1).start()

    def gathered(j):
        for r in range(2):

            @pl.when(((rep == 1) & (j == n - 1)) == (r == 1))
            def _():
                some = w.at[j, pl.ds(0, SPLIT + r)]
                across(some, some, as_sem.at[0], ar_sem.at[j]).wait_recv()

    halves = 2
    half = tokens // halves

    def gather(far, part_of, ends=None):
        at_rows = pl.ds(pl.multiple_of(part_of * half, half), half)
        for d in range(2):
            here = at[d] >= far
            if ends is not None:
                here &= (at[d] == n - 1) == ends

            @pl.when(here)
            def _():
                j = k - sign[d] * far

                @pl.when(part_of == 0)
                def _():
                    gathered(j)
                    if ends:
                        deferred(d).wait_recv()

                dhid[at_rows, :] += multiply(j, at_rows)

    for s in range(1, n - 1):
        steps(0, end, functools.partial(pass_on, s))
    steps(0, end, functools.partial(pass_on, n - 1))
    for d in range(2):

        @pl.when(at[d] == n - 2)
        def _():
            deferred(d).start()

    def put(p, m, value, lanes):
        gd[pl.ds(p, m)] = value
        if lanes is not None:
            sq = value * value
            total = sq[:, :, :128]
            for b in range(1, cols // 128):
                total += sq[:, :, b * 128 : (b + 1) * 128]
            lanes[pl.ds(p, m)] = total

    def finish(c, m, i):
        p = piece(c)
        some = pl.ds(c, m)

        @pl.when(c == free)
        def _():
            early(k).wait_recv()

        @pl.when(c >= free)
        def _():
            part[k, pl.ds(p, m)] += yrecv[k, pl.ds(jnp.maximum(c - free, 0), m)].astype(F32)

        for d in range(2):

            @pl.when(at[d] > 0)
            def _():
                along(d, n - 1, i, zsend.at[d, n - 2, some], zrecv.at[d, n - 2, some]).wait_recv()
                part[k, pl.ds(p, m)] += zrecv[d, n - 2, some].astype(F32)

        fsend[some] = part[k, pl.ds(p, m)].astype(BF16)
        final(c, m, i).start()

        @pl.when(c >= free)
        def _():
            put(p, m, fsend[some].astype(F32) * factor, lanes_s)

    def deliver(c, m, i):
        some = pl.ds(c, m)

        @pl.when(c < free)
        def _():
            put(piece(c), m, (fsend[some].astype(F32) + frecv[some].astype(F32)) * factor, lanes_u)

        @pl.when(c >= free)
        def _():
            put(mate * SPLIT + c - free, m, frecv[some].astype(F32) * factor, None)

    def energy(lanes):
        return jnp.sum(lanes[...].reshape(hidden_units, 128).T, axis=0, keepdims=True)

    def free_energy(to, slot):
        return pltpu.make_async_remote_copy(
            src_ref=esu, dst_ref=eru.at[slot], send_sem=us_sem.at[0], recv_sem=ur_sem.at[0],
            device_id={"fs": to}, device_id_type=MESH,
        )

    def split_energy(other, to, slot):
        return pltpu.make_async_remote_copy(
            src_ref=ess, dst_ref=ers.at[rep, slot], send_sem=ss_sem.at[other], recv_sem=sr_sem.at[other],
            device_id={"rep": jnp.where(other == 1, mate, rep), "fs": to}, device_id_type=MESH,
        )

    blocks = 4
    brows = tokens // blocks

    def activations(i):
        at_rows = pl.ds(pl.multiple_of(i * brows, brows), brows)
        gate = g[at_rows, :].astype(F32)
        up = u[at_rows, :].astype(F32)
        grad = dhid[at_rows, :]
        sig = jax.nn.sigmoid(gate)
        du[at_rows, :] = (grad * (gate * sig)).astype(BF16)
        dg[at_rows, :] = (grad * up * sig * (1.0 + gate * (1.0 - sig))).astype(BF16)

    def last(c, m, i):
        finish(c, m, i)

        @pl.when((i >= FROM) & (i < FROM + halves))
        def _():
            gather(1, i - FROM, ends=False)

        @pl.when((i >= FROM + halves) & (i < FROM + halves + n - 2))
        def _():
            loop(0, halves, functools.partial(gather, 2 + i - FROM - halves))

    steps(0, end - 1, last)
    steps(end - 1, end, finish)
    ess[...] = energy(lanes_s)
    for t in range(1, n):
        split_energy(0, lax.rem(k + t, n), k).start()
    for t in range(n):
        split_energy(1, lax.rem(k + t, n), k).start()

    def outputs():
        @pl.when((k == 0) | (k == n - 1))
        def _():
            loop(0, halves, functools.partial(gather, 1, ends=True))

        loop(0, blocks, activations)

    @pl.when(rep == FIRST)
    def _():
        outputs()

    def arrived(start, pieces, slot):
        some = pl.ds(start, pieces)
        across(fsend.at[some], frecv.at[some], fs_sem.at[0], fr_sem.at[slot]).wait_recv()

    arrived(0, free, 0)
    steps(0, free // GROUP, deliver)
    base = 2 * SPLIT * rows // 128 * 128
    base = base if base % rows == 0 else 0
    tail = lanes_u[base // rows :].reshape(hidden_units - base, 128)
    esu[:, base:] = jnp.sum(tail.T, axis=0, keepdims=True)
    for t in range(1, n):
        free_energy(lax.rem(k + t, n), k).start()

    @pl.when(rep != FIRST)
    def _():
        outputs()

    arrived(free, SPLIT, 1)
    steps(free // GROUP, end, deliver)

    for d in range(2):

        for p in range(n - 1):
            for r in range(2):

                @pl.when((at[d] == p) & (rep == r))
                def _():
                    sent = spread((p + 1) * count - r * d)
                    along(d, 0, 0, sent, sent).wait_send()
                    sent = zsend.at[d, pl.ds(0, n - 1 - p)]
                    along(d, 0, 0, sent, sent, 1).wait_send()

    across(fsend, frecv, fs_sem.at[0], fr_sem.at[0]).wait_send()
    across(ysend, yrecv, ys_sem.at[0], yr_sem.at[0]).wait_send()

    for r in range(2):

        @pl.when(((rep == 0) & (k < n - 1)) == (r == 1))
        def _():
            crossed = spread((n - 1) * SPLIT + r)
            across(crossed, crossed, as_sem.at[0], ar_sem.at[0]).wait_send()

    def settle(some, send, recv):
        copy = across(some, some, send, recv)
        copy.wait_send()
        copy.wait_recv()

    settle(eru.at[pl.ds(0, n - 1)], us_sem.at[0], ur_sem.at[0])
    settle(ers.at[0, pl.ds(0, n - 1)], ss_sem.at[0], sr_sem.at[0])
    settle(ers.at[1], ss_sem.at[1], sr_sem.at[1])
    total = jnp.zeros((1, hidden_units), F32)
    for j in range(n):
        total += jnp.where(j == k, esu[...], eru[j])
        for r in range(2):
            total += jnp.where((j == k) & (r == rep), ess[...], ers[r, j])
    en_ref[...] = total * (1.0 / width)


def write_out(dg, du, gd, en, dg_hbm, du_hbm, gd_hbm, en_hbm, flat, sem):
    def copy_of(i, src, dst):
        return pltpu.make_async_copy(src, dst, sem.at[i])

    copies = [copy_of(0, dg, dg_hbm), copy_of(1, du, du_hbm), copy_of(2, gd, gd_hbm)]
    for copy in copies:
        copy.start()
    flat[...] = en[0, :]
    copies.append(copy_of(3, flat, en_hbm))
    copies[3].start()
    for copy in copies:
        copy.wait()


def fused(n, gate_pre, up_pre, out_grad, w_down):
    tokens, units = gate_pre.shape
    width = out_grad.shape[1]
    cols = w_down.shape[1]
    rows = units // PIECES
    count = PIECES - SPLIT
    factor = float(tokens * lax.axis_size("rep") * n) ** (-0.5)
    any_spec = pl.BlockSpec(memory_space=pl.ANY)
    vmem_spec = pl.BlockSpec(memory_space=pltpu.VMEM)
    dma = pltpu.SemaphoreType.DMA
    d_gate, d_up, grad, energy = pl.pallas_call(
        functools.partial(kernel, n, factor, width),
        out_shape=(
            pltpu.VMEM((tokens, units), BF16),
            pltpu.VMEM((tokens, units), BF16),
            pltpu.VMEM((PIECES, rows, cols), F32),
            pltpu.VMEM((1, units), F32),
        ),
        in_specs=[any_spec] * 4,
        out_specs=(vmem_spec,) * 4,
        scratch_shapes=[
            pltpu.VMEM((tokens, units), BF16),
            pltpu.VMEM((tokens, units), BF16),
            pltpu.VMEM((n, tokens, cols), BF16),
            pltpu.VMEM((n, PIECES, rows, cols), BF16),
            pltpu.VMEM((units, tokens), BF16),
            pltpu.VMEM((n, PIECES, rows, cols), F32),
            pltpu.VMEM((tokens, units), F32),
            pltpu.VMEM((2, n - 1, count, rows, cols), BF16),
            pltpu.VMEM((2, n - 1, count, rows, cols), BF16),
            pltpu.VMEM((n, SPLIT, rows, cols), BF16),
            pltpu.VMEM((n, SPLIT, rows, cols), BF16),
            pltpu.VMEM((count, rows, cols), BF16),
            pltpu.VMEM((count, rows, cols), BF16),
            pltpu.VMEM((PIECES, rows, 128), F32),
            pltpu.VMEM((PIECES, rows, 128), F32),
            pltpu.VMEM((1, units), F32),
            pltpu.VMEM((n, 1, units), F32),
            pltpu.VMEM((1, units), F32),
            pltpu.VMEM((2, n, 1, units), F32),
            dma((3 + LOADS,)),
            dma((n,)),
            dma((2, 2)),
            dma((2, 2 * -(-count // GROUP) + 1)),
            dma((2,)),
            dma((1,)),
            dma((n,)),
            dma((1,)),
            dma((n,)),
            dma((1,)),
            dma((2,)),
            dma((1,)),
            dma((1,)),
            dma((2,)),
            dma((2,)),
        ],
        compiler_params=pltpu.CompilerParams(
            collective_id=0, has_side_effects=True, vmem_limit_bytes=VMEM_LIMIT
        ),
    )(gate_pre, up_pre, out_grad, w_down.reshape(PIECES, rows, cols))
    return pl.pallas_call(
        write_out,
        out_shape=(
            jax.ShapeDtypeStruct((tokens, units), BF16),
            jax.ShapeDtypeStruct((tokens, units), BF16),
            jax.ShapeDtypeStruct((units, cols), F32),
            jax.ShapeDtypeStruct((units,), F32),
        ),
        in_specs=[vmem_spec] * 4,
        out_specs=(any_spec,) * 4,
        scratch_shapes=[pltpu.VMEM((units,), F32), dma((4,))],
        compiler_params=pltpu.CompilerParams(vmem_limit_bytes=4 * 1024 * 1024),
    )(d_gate, d_up, grad.reshape(units, cols), energy)


def solution(mesh):
    reps, n = mesh.shape["rep"], mesh.shape["fs"]

    def local(gate_pre, up_pre, out_grad, w_down):
        units, cols = w_down.shape
        fits = reps == 2 and 2 <= n <= 4 and cols % 128 == 0 and units % (PIECES * 16) == 0 and units % 128 == 0
        if fits and gate_pre.shape[0] % 1024 == 0:
            return fused(n, gate_pre, up_pre, out_grad, w_down)
        return plain(gate_pre, up_pre, out_grad, w_down)

    placed = (P(("rep", "fs"), "tp"), P(("rep", "fs"), "tp"), P(("rep", "fs"), None), P("tp", "fs"))
    return jax.shard_map(
        local,
        mesh=mesh,
        in_specs=placed,
        out_specs=(P(("rep", "fs"), "tp"), P(("rep", "fs"), "tp"), P("tp", "fs"), P("tp")),
        check_vma=False,
    )
```
